128 devices in a mesh: fs: 16 (over z, x), tp: 8 (over y, core).
Axes of the slice: x: 4, y: 4, z: 4, core: 2. Of those that a mesh axis runs over, the one named last changes fastest.
Arguments:
- tokens: bfloat16 [16384, 2048], P('fs', 'tp'), may hold values from -6 to 6
- recurrence_norm_gain: float32 [2048], replicated, may hold values from 0.1 to 1.9
- output_gate_weight: bfloat16 [2048, 2816], P('fs', 'tp'), may hold values from -0.125 to 0.125
- recurrence_input_weight: bfloat16 [2048, 2816], P('fs', 'tp'), may hold values from -0.125 to 0.125
- convolution_taps: float32 [4, 2816], P(None, 'tp'), may hold values from -3 to 3
- recurrence_gate_weight: bfloat16 [8, 352, 352], P('tp'), may hold values from -0.3125 to 0.3125
- input_gate_weight: bfloat16 [8, 352, 352], P('tp'), may hold values from -0.3125 to 0.3125
- base_decay_logit: float32 [2816], P('tp'), may hold values from 4.5 to 9.5
- token_log_decay: float32 [16384], P('fs'), may hold values from -0.7 to 0, as said below
- recurrence_output_weight: bfloat16 [2816, 2048], P('tp', 'fs'), may hold values from -0.4375 to 0.4375
- feedforward_norm_gain: float32 [2048], replicated, may hold values from 0.1 to 1.9
- feedforward_gate_weight: bfloat16 [2048, 5632], P('fs', 'tp'), may hold values from -0.125 to 0.125
- feedforward_up_weight: bfloat16 [2048, 5632], P('fs', 'tp'), may hold values from -0.125 to 0.125
- feedforward_down_weight: bfloat16 [5632, 2048], P('tp', 'fs'), may hold values from -0.15625 to 0.15625
Outputs:
- layer_out: bfloat16 [16384, 2048], P('fs', 'tp')
The draws below stay inside these ranges and needn't reach their ends.
Inputs may be any that keep to these rules, and one draw needn't show every extreme that they name: `token_log_decay`: each entry is zero or lies between -0.7 and -0.22.
All inputs are finite; a program needn't handle non-finite values.
Results may differ from the reference program's by a relative error of at most 0.022.
Values may be sent and summed in bfloat16 or wider, within the bound.
A program may use at most 128 MiB of HBM per device.

```python
import jax
import jax.numpy as jnp
from jax import lax

D = 2048
R = 2816
BW = 352
FF = 5632
CONV = 4
LEN = 128
BLOCKS = 8
TOKENS = 16384
N_TP = 8


def draw_base_decay_logit(key, part):
    keys = jax.random.split(jax.random.fold_in(key, 11), 3)
    slower = jax.random.bernoulli(keys[0], 0.5, (R,))
    fast_values = jax.random.uniform(keys[1], (R,), jnp.float32, 4.5, 5.5)
    slow_values = jax.random.uniform(keys[2], (R,), jnp.float32, 6.5, 9.0)
    return jnp.where(slower, slow_values, fast_values)


def draw_token_log_decay(key, part):
    keys = jax.random.split(jax.random.fold_in(key, 23), 2)
    struck = jax.random.bernoulli(keys[0], 3.0 / LEN, (TOKENS,))
    depths = jax.random.uniform(keys[1], (TOKENS,), jnp.float32, -0.7, -0.22)
    return jnp.where(struck, depths, jnp.zeros((TOKENS,), jnp.float32))


def levels(stream_key, extent, shards, smallest, largest):
    loudness, own = 1.0, jax.random.fold_in(stream_key, 6)
    for axis_at, shards_of in shards:
        heights = jnp.exp(jax.random.uniform(jax.random.fold_in(own, axis_at), (shards_of,), jnp.float32, smallest / len(shards), largest / len(shards)))
        loudness = loudness * jnp.repeat(heights, extent[axis_at] // shards_of).reshape([-1 if axis == axis_at else 1 for axis in range(len(extent))])
    return loudness


def scatter_about(key, dims, deviation, limit, pieces=(), kind=jnp.bfloat16):
    entries = jax.random.normal(key, dims, jnp.float32) * deviation
    if len(pieces) > 0:
        entries = levels(key, dims, pieces, -0.22, 0.18) * entries
    return jnp.clip(entries, min=-limit, max=limit).astype(kind)


def setup_inputs(seed: int = 0) -> dict:
    arg_keys = jax.random.split(jax.random.key(seed), 15)
    return {
        "tokens": scatter_about(arg_keys[0], (TOKENS, D), 1.0, 6.0, ((0, 16), (1, 8))),
        "recurrence_norm_gain": jnp.clip(1.0 + 0.18 * jax.random.normal(arg_keys[1], (D,), jnp.float32), 0.1, 1.9),
        "output_gate_weight": scatter_about(arg_keys[2], (D, R), D ** -0.5, 0.125, ((0, 16), (1, 8))),
        "recurrence_input_weight": scatter_about(arg_keys[3], (D, R), D ** -0.5, 0.125, ((0, 16), (1, 8))),
        "convolution_taps": scatter_about(arg_keys[4], (CONV, R), CONV ** -0.5, 3.0, ((1, 8),), jnp.float32),
        "recurrence_gate_weight": scatter_about(arg_keys[5], (BLOCKS, BW, BW), BW ** -0.5, 0.3125, ((0, 8),)),
        "input_gate_weight": scatter_about(arg_keys[6], (BLOCKS, BW, BW), BW ** -0.5, 0.3125, ((0, 8),)),
        "base_decay_logit": draw_base_decay_logit(jax.random.fold_in(arg_keys[14], 71), 0),
        "token_log_decay": draw_token_log_decay(jax.random.fold_in(arg_keys[14], 71), 0),
        "recurrence_output_weight": scatter_about(arg_keys[9], (R, D), (R // 16) ** -0.5, 0.4375, ((0, 8), (1, 16))),
        "feedforward_norm_gain": jnp.clip(1.0 + 0.18 * jax.random.normal(arg_keys[10], (D,), jnp.float32), 0.1, 1.9),
        "feedforward_gate_weight": scatter_about(arg_keys[11], (D, FF), D ** -0.5, 0.125, ((0, 16), (1, 8))),
        "feedforward_up_weight": scatter_about(arg_keys[12], (D, FF), D ** -0.5, 0.125, ((0, 16), (1, 8))),
        "feedforward_down_weight": scatter_about(arg_keys[13], (FF, D), (FF // 4) ** -0.5, 0.15625, ((0, 8), (1, 16))),
    }


EPSILON = 1e-06
GATE_EXPONENT = 8.0

def norm_rows(values, gain_vec):
    widened = values.astype(jnp.float32)
    scaled = widened * lax.rsqrt(lax.optimization_barrier(jnp.mean(widened * widened, axis=-1, keepdims=True)) + EPSILON)
    return (scaled * gain_vec).astype(jnp.bfloat16)

def causal_taps(feature_vector, convolution_taps, length):
    row_count, channels = feature_vector.shape
    blocks = feature_vector.astype(jnp.float32).reshape(row_count // length, length, channels)
    tap_count = convolution_taps.shape[0]
    padded = jnp.pad(blocks, ((0, 0), (tap_count - 1, 0), (0, 0)))
    summed = jnp.zeros_like(blocks)
    for offset in range(tap_count):
        summed = summed + convolution_taps[offset] * padded[:, offset:offset + length]
    return summed.reshape(row_count, channels).astype(jnp.bfloat16)

def combine_steps(earlier, latter):
    return (earlier[0] * latter[0], latter[0] * earlier[1] + latter[1])

def linear_scan(decays, driven, length):
    row_count, channels = decays.shape
    shaped = (decays.reshape(row_count // length, length, channels), driven.reshape(row_count // length, length, channels))
    result = lax.associative_scan(combine_steps, shaped, axis=1)
    return result[1].reshape(row_count, channels)

def block_map(mixed_in, weight):
    row_count = mixed_in.shape[0]
    shaped = mixed_in.astype(jnp.float32).reshape(row_count, BLOCKS, BW)
    return jnp.einsum('tnd,nde->tne', shaped, weight.astype(jnp.float32)).reshape(row_count, R)

def grouped_product(values, weight, group_count):
    step_size = values.shape[1] // group_count
    summed = jnp.zeros((values.shape[0], weight.shape[1]), jnp.float32)
    for group_index in range(group_count):
        lower = group_index * step_size
        partial_product = jnp.dot(values[:, lower:lower + step_size], weight[lower:lower + step_size], preferred_element_type=jnp.float32).astype(jnp.bfloat16)
        summed = summed + lax.optimization_barrier(partial_product).astype(jnp.float32)
    return summed

def reference(tokens, recurrence_norm_gain, output_gate_weight, recurrence_input_weight, convolution_taps, recurrence_gate_weight, input_gate_weight, base_decay_logit, token_log_decay, recurrence_output_weight, feedforward_norm_gain, feedforward_gate_weight, feedforward_up_weight, feedforward_down_weight):
    normed = norm_rows(tokens, recurrence_norm_gain)
    gate_projected = jnp.dot(normed, output_gate_weight, preferred_element_type=jnp.float32)
    feature_vector = jnp.dot(normed, recurrence_input_weight, preferred_element_type=jnp.float32).astype(jnp.bfloat16)
    mixed_in = causal_taps(feature_vector, convolution_taps, LEN)
    recurrence_gate = jax.nn.sigmoid(block_map(mixed_in, recurrence_gate_weight))
    inject_gate = jax.nn.sigmoid(block_map(mixed_in, input_gate_weight))
    decay_log_value = -GATE_EXPONENT * jax.nn.softplus(-base_decay_logit)[None, :] * recurrence_gate + token_log_decay[:, None]
    decays = jnp.exp(decay_log_value)
    driven = jnp.sqrt(-jnp.expm1(2.0 * decay_log_value)) * (inject_gate * mixed_in.astype(jnp.float32))
    states = linear_scan(decays, driven, LEN)
    carried = (states * jax.nn.gelu(gate_projected)).astype(jnp.bfloat16)
    mixer_sum = grouped_product(carried, recurrence_output_weight, N_TP)
    residual = (tokens.astype(jnp.float32) + mixer_sum).astype(jnp.bfloat16)
    normed_two = norm_rows(residual, feedforward_norm_gain)
    gate_hidden = jnp.dot(normed_two, feedforward_gate_weight, preferred_element_type=jnp.float32)
    up_hidden = jnp.dot(normed_two, feedforward_up_weight, preferred_element_type=jnp.float32)
    hidden = (jax.nn.silu(gate_hidden) * up_hidden).astype(jnp.bfloat16)
    hidden_sum = grouped_product(hidden, feedforward_down_weight, N_TP)
    return (residual.astype(jnp.float32) + hidden_sum).astype(jnp.bfloat16)
```

```python
import functools

import jax
import jax.numpy as jnp
from jax import lax
from jax.experimental import pallas as pl
from jax.experimental.pallas import tpu as pltpu
from jax.sharding import PartitionSpec as P

MESH = pl.DeviceIdType.MESH
F32 = jnp.float32
BF16 = jnp.bfloat16

LEN = 128
EPSILON = 1e-06
GATE_EXPONENT = 8.0

SIDE = 4
CHUNKS = 4
ROWS = 1024
CH = ROWS // CHUNKS
HALF = CH // 2
SEQS = 8
RP = 384
FFL = 704
GU = 640
CB = 256


def row_ranges(kind):
    if kind == "row":
        return {0: ((0, 32), (32, 32)), 1: ((64, 32), (96, 32))}
    if kind == "wo":
        return {0: ((0, 96), (96, 80)), 1: ((176, 96), (272, 80))}
    return {0: ((0, 176), (176, 176)), 1: ((352, 176), (528, 176))}


class Gather:
    def __init__(self, buf, kind, send, recv, pos, dev):
        self.buf, self.kind, self.send, self.recv, self.pos, self.dev = buf, kind, send, recv, pos, dev
        self.rows = row_ranges(kind)

    def span(self, part, half):
        lo, hi = self.rows[part]
        if half == 0:
            return pl.ds(lo[0], lo[1])
        if half == 1:
            return pl.ds(hi[0], hi[1])
        return pl.ds(lo[0], lo[1] + hi[1])

    def block(self, part, i1, i2, half=None):
        z, x = (i2, i1) if part == 0 else (i1, i2)
        rows = self.span(part, half)
        if self.kind == "row":
            return self.buf.at[z, x, rows, :]
        cols = pl.ds(pl.multiple_of(lax.rem(x, 2) * 128, 128), 128)
        return self.buf.at[z, x // 2, rows, cols]

    def line(self, part, i2, half=None):
        rows = self.span(part, None)
        if part == 0:
            if self.kind == "row":
                xs = pl.ds(0, 4) if half is None else pl.ds(2 * half, 2)
            else:
                xs = pl.ds(0, 2) if half is None else pl.ds(half, 1)
            return self.buf.at[i2, xs, rows, :]
        zs = pl.ds(0, 4) if half is None else pl.ds(2 * half, 2)
        if self.kind == "row":
            return self.buf.at[zs, i2, rows, :]
        cols = pl.ds(pl.multiple_of(lax.rem(i2, 2) * 128, 128), 128)
        return self.buf.at[zs, i2 // 2, rows, cols]

    def copy(self, view, part, k, to):
        return pltpu.make_async_remote_copy(
            src_ref=view,
            dst_ref=view,
            send_sem=self.send.at[part, k],
            recv_sem=self.recv.at[part, k],
            device_id=to,
            device_id_type=MESH,
        )

    def around(self, part):
        a1, a2 = ("x", "z") if part == 0 else ("z", "x")
        return a1, a2, self.pos[a1], self.pos[a2]

    def moves(self, part):
        a1, a2, (m1, i1, p1), (m2, i2, p2) = self.around(part)
        far1, far2 = lax.rem(i1 + 2, SIDE), lax.rem(i2 + 2, SIDE)
        return [
            self.block(part, m1, i2),
            self.block(part, p1, i2),
            self.block(part, far1, i2, 0),
            self.block(part, far1, i2, 1),
            self.line(part, m2),
            self.line(part, p2),
            self.line(part, far2, 0),
            self.line(part, far2, 1),
        ]

    def arrived(self, part, k):
        self.copy(self.moves(part)[k], part, k, self.dev["x"][0]).wait_recv()

    def stage0(self):
        for part in (0, 1):
            a1, a2, (m1, i1, p1), (m2, i2, p2) = self.around(part)
            view = self.block(part, i1, i2)
            self.copy(view, part, 0, self.dev[a1][1]).start()
            self.copy(view, part, 1, self.dev[a1][0]).start()

    def stage1(self):
        for part in (0, 1):
            a1, a2, (m1, i1, p1), (m2, i2, p2) = self.around(part)
            self.arrived(part, 0)
            self.copy(self.block(part, m1, i2, 0), part, 2, self.dev[a1][1]).start()
            self.arrived(part, 1)
            self.copy(self.block(part, p1, i2, 1), part, 3, self.dev[a1][0]).start()

    def stage2(self):
        for part in (0, 1):
            a1, a2, (m1, i1, p1), (m2, i2, p2) = self.around(part)
            self.arrived(part, 2)
            self.arrived(part, 3)
            view = self.line(part, i2)
            self.copy(view, part, 4, self.dev[a2][1]).start()
            self.copy(view, part, 5, self.dev[a2][0]).start()

    def stage3(self):
        for part in (0, 1):
            a1, a2, (m1, i1, p1), (m2, i2, p2) = self.around(part)
            self.arrived(part, 4)
            self.copy(self.line(part, m2, 0), part, 6, self.dev[a2][1]).start()
            self.arrived(part, 5)
            self.copy(self.line(part, p2, 1), part, 7, self.dev[a2][0]).start()

    def stage4(self):
        for part in (0, 1):
            self.arrived(part, 6)
            self.arrived(part, 7)

    def drain(self):
        for part in (0, 1):
            for k, view in enumerate(self.moves(part)):
                self.copy(view, part, k, self.dev["x"][0]).wait_send()


class Spread:
    def __init__(self, buf, send, recv, y, core, dev):
        self.buf, self.send, self.recv, self.dev = buf, send, recv, dev
        (ym, yy, yp), far = y, lax.rem(y[1] + 2, SIDE)
        other = 1 - core
        self.own, self.minus, self.plus, self.far = (2 * v + core for v in (yy, ym, yp, far))
        self.others = [2 * v + other for v in (yy, ym, yp, far)]

    def view(self, block, c, half=None):
        if half is None:
            return self.buf.at[block, pl.ds(pl.multiple_of(c * CH, CH), CH), :]
        return self.buf.at[block, pl.ds(pl.multiple_of(c * CH + half * HALF, HALF), HALF), :]

    def copy(self, view, k, c, to):
        return pltpu.make_async_remote_copy(
            src_ref=view,
            dst_ref=view,
            send_sem=self.send.at[k, c],
            recv_sem=self.recv.at[k, c],
            device_id=to,
            device_id_type=MESH,
        )

    def landing(self, k, c):
        return [
            (self.minus, None),
            (self.plus, None),
            (self.others[0], None),
            (self.far, 0),
            (self.far, 1),
            (self.others[1], None),
            (self.others[2], None),
            (self.others[3], None),
        ][k]

    def arrived(self, k, c):
        block, half = self.landing(k, c)
        self.copy(self.view(block, c, half), k, c, self.dev["core"]).wait_recv()

    def stage0(self, c):
        view = self.view(self.own, c)
        self.copy(view, 0, c, self.dev["y"][1]).start()
        self.copy(view, 1, c, self.dev["y"][0]).start()
        self.copy(view, 2, c, self.dev["core"]).start()

    def stage1(self, c):
        self.arrived(0, c)
        self.copy(self.view(self.minus, c, 0), 3, c, self.dev["y"][1]).start()
        self.copy(self.view(self.minus, c), 5, c, self.dev["core"]).start()
        self.arrived(1, c)
        self.copy(self.view(self.plus, c, 1), 4, c, self.dev["y"][0]).start()
        self.copy(self.view(self.plus, c), 6, c, self.dev["core"]).start()

    def stage2(self, c):
        self.arrived(3, c)
        self.arrived(4, c)
        self.copy(self.view(self.far, c), 7, c, self.dev["core"]).start()

    def stage3(self, c):
        for k in (2, 5, 6, 7):
            self.arrived(k, c)

    def drain(self, c):
        for k in range(8):
            block, half = self.landing(k, c)
            self.copy(self.view(block, c, half), k, c, self.dev["core"]).wait_send()


class Sum:
    def __init__(self, give, keep, took, total, halves, finals, send, recv, y, core, dev):
        self.give, self.keep, self.took, self.total = give, keep, took, total
        self.halves, self.finals, self.send, self.recv, self.dev = halves, finals, send, recv, dev
        self.minus, self.own, self.plus = y
        self.far = lax.rem(y[1] + 2, SIDE)

    def rows(self, c):
        return pl.ds(pl.multiple_of(c * CH, CH), CH)

    def half(self, c, h):
        return pl.ds(pl.multiple_of(c * CH + h * HALF, HALF), HALF)

    def parts(self, k, c):
        if k == 0:
            return self.give.at[:, self.rows(c), :], self.took.at[:, self.rows(c), :], self.dev["core"]
        if k <= 2:
            return self.total.at[self.far, self.half(c, k - 1), :], self.halves.at[k - 1, c], self.dev["y"][2 - k]
        to = self.plus if k == 3 else self.minus
        return self.total.at[to, self.rows(c), :], self.finals.at[k - 3, self.rows(c), :], self.dev["y"][4 - k]

    def copy(self, k, c):
        src, dst, to = self.parts(k, c)
        return pltpu.make_async_remote_copy(
            src_ref=src,
            dst_ref=dst,
            send_sem=self.send.at[k, c],
            recv_sem=self.recv.at[k, c],
            device_id=to,
            device_id_type=MESH,
        )

    def stage0(self, c):
        self.copy(0, c).start()

    def stage1(self, c):
        self.copy(0, c).wait_recv()
        rows = self.rows(c)
        for target in (self.far, self.plus, self.minus, self.own):
            self.total[target, rows, :] = (
                self.keep[target, rows, :].astype(F32) + self.took[target, rows, :].astype(F32)
            ).astype(BF16)
        self.copy(1, c).start()
        self.copy(2, c).start()

    def stage2(self, c):
        for h, target in ((0, self.plus), (1, self.minus)):
            self.copy(1 + h, c).wait_recv()
            rows = self.half(c, h)
            self.total[target, rows, :] = (
                self.total[target, rows, :].astype(F32) + self.halves[h, c].astype(F32)
            ).astype(BF16)
        self.copy(3, c).start()
        self.copy(4, c).start()

    def stage3(self, c):
        self.copy(3, c).wait_recv()
        self.copy(4, c).wait_recv()
        rows = self.rows(c)
        return (
            self.total[self.own, rows, :].astype(F32)
            + self.finals[0, rows, :].astype(F32)
            + self.finals[1, rows, :].astype(F32)
        )

    def drain(self, c):
        for k in range(5):
            self.copy(k, c).wait_send()


def norm_chunk(full, gain, out, c):
    step = 16

    def body(i, carry):
        rows = pl.ds(pl.multiple_of(c * CH + i * step, step), step)
        here = pl.ds(pl.multiple_of(i * step, step), step)
        total = jnp.zeros((step, CB), F32)
        for b in range(8):
            v = full[b, rows, :].astype(F32)
            total = total + v * v
        scale = lax.rsqrt(jnp.sum(total, axis=1, keepdims=True) * (1.0 / 2048.0) + EPSILON)
        for b in range(8):
            v = full[b, rows, :].astype(F32)
            out[here, b * CB : (b + 1) * CB] = ((v * scale) * gain[b : b + 1, :]).astype(BF16)
        return carry

    lax.fori_loop(0, CH // step, body, 0, unroll=2)


def kernel(
    tok_hbm, wgi_hbm, wo_hbm, wff_hbm, wd_hbm, gm, small, ld, gain1, gain2,
    out,
    full1, full2, wgi, wo, wff, wd,
    give1, keep1, took1, total1, halves1, finals1,
    give2, keep2, took2, total2, halves2, finals2,
    feat, proj, mixed, gl, carried, nrm, ffo, hid, state,
    local_sem, w_send, w_recv, a_send, a_recv, s_send, s_recv,
):
    fs, tp = lax.axis_index("fs"), lax.axis_index("tp")
    iz, ix = fs // SIDE, lax.rem(fs, SIDE)
    iy, core = tp // 2, lax.rem(tp, 2)

    def ring(i):
        return lax.rem(i + SIDE - 1, SIDE), i, lax.rem(i + 1, SIDE)

    pos = {"x": ring(ix), "z": ring(iz)}
    y = ring(iy)
    dev = {
        "x": tuple({"fs": iz * SIDE + pos["x"][k]} for k in (0, 2)),
        "z": tuple({"fs": pos["z"][k] * SIDE + ix} for k in (0, 2)),
        "y": tuple({"tp": 2 * y[k] + core} for k in (0, 2)),
        "core": {"tp": 2 * iy + 1 - core},
    }

    barrier = pltpu.get_barrier_semaphore()
    for to in (*dev["x"], *dev["z"], *dev["y"], dev["core"]):
        pl.semaphore_signal(barrier, inc=1, device_id=to, device_id_type=MESH)

    cols = pl.ds(pl.multiple_of(lax.rem(ix, 2) * 128, 128), 128)
    own = [
        pltpu.make_async_copy(wgi_hbm, wgi.at[iz, ix], local_sem.at[0]),
        pltpu.make_async_copy(tok_hbm, full1.at[tp], local_sem.at[1]),
        pltpu.make_async_copy(wo_hbm, wo.at[iz, ix // 2, pl.ds(0, 352), cols], local_sem.at[2]),
        pltpu.make_async_copy(wff_hbm, wff.at[iz, ix], local_sem.at[3]),
        pltpu.make_async_copy(wd_hbm, wd.at[iz, ix // 2, :, cols], local_sem.at[4]),
    ]
    for copy in own:
        copy.start()
    wo[:, :, 352:RP, :] = jnp.zeros((SIDE, 2, RP - 352, CB), BF16)
    feat[0:24, :] = jnp.zeros((24, RP), F32)
    state[...] = jnp.zeros_like(state)

    gathers = [
        Gather(buf, kind, w_send.at[m], w_recv.at[m], pos, dev)
        for m, (buf, kind) in enumerate(((wgi, "row"), (wo, "wo"), (wff, "row"), (wd, "wd")))
    ]
    g_wgi, g_wo, g_wff, g_wd = gathers
    spread1 = Spread(full1, a_send.at[0], a_recv.at[0], y, core, dev)
    spread2 = Spread(full2, a_send.at[1], a_recv.at[1], y, core, dev)
    sum1 = Sum(give1, keep1, took1, total1, halves1, finals1, s_send.at[0], s_recv.at[0], y, core, dev)
    sum2 = Sum(give2, keep2, took2, total2, halves2, finals2, s_send.at[1], s_recv.at[1], y, core, dev)

    pl.semaphore_wait(barrier, 7)

    def each_chunk(stage):
        def body(c, carry):
            stage(c)
            return carry

        lax.fori_loop(0, CHUNKS, body, 0)

    own[0].wait()
    g_wgi.stage0()
    own[1].wait()
    each_chunk(spread1.stage0)
    own[2].wait()
    g_wo.stage0()
    own[3].wait()
    g_wff.stage0()
    own[4].wait()
    g_wd.stage0()
    g_wgi.stage1()
    g_wo.stage1()
    each_chunk(spread1.stage1)
    g_wff.stage1()
    g_wgi.stage2()
    g_wo.stage2()
    g_wd.stage1()
    each_chunk(spread1.stage2)
    g_wff.stage2()
    g_wd.stage2()
    g_wgi.stage3()
    g_wo.stage3()
    each_chunk(spread1.stage3)
    g_wgi.stage4()

    def mix(c):
        norm_chunk(full1, gain1, nrm, c)
        base = pl.multiple_of(c * CH, CH)
        projected = jnp.dot(nrm[...], wgi[...].reshape(2048, 2 * RP), preferred_element_type=F32)
        proj[...] = projected[:, :RP]
        feat[pl.ds(base + 24, CH), :] = projected[:, RP:].astype(BF16).astype(F32)

        def taps(i, carry):
            r = pl.multiple_of(i * 32, 32)
            summed = small[0:1, :] * feat[pl.ds(base + r, 32), :]
            for k in range(1, 4):
                summed = summed + small[k : k + 1, :] * feat[pl.ds(base + r + 8 * k, 32), :]
            mixed[pl.ds(r, 32), :] = summed.astype(BF16)
            return carry

        lax.fori_loop(0, CH // 32, taps, 0, unroll=2)
        gl[...] = jnp.dot(mixed[...], gm[...], preferred_element_type=F32)

        def steps(i, h):
            r = pl.multiple_of(i * 32, 32)
            rows = pl.ds(r, 32)
            recur = jax.nn.sigmoid(gl[rows, :RP])
            inject = jax.nn.sigmoid(gl[rows, RP:])
            log_decay = small[4:5, :] * recur + ld[pl.ds(base + r, 32), :]
            decay = jnp.exp(log_decay)
            twice = 2.0 * log_decay
            near = -twice * (1.0 + twice * (0.5 + twice * (1.0 / 6.0 + twice * (1.0 / 24.0 + twice * (1.0 / 120.0)))))
            rest = jnp.where(twice > -0.1, near, 1.0 - decay * decay)
            driven = jnp.sqrt(rest) * (inject * mixed[rows, :].astype(F32))
            states = []
            for s in range(4):
                h = decay[8 * s : 8 * s + 8] * h + driven[8 * s : 8 * s + 8]
                states.append(h)
            carried[rows, :] = (jnp.concatenate(states, axis=0) * jax.nn.gelu(proj[rows, :])).astype(BF16)
            return h

        state[...] = lax.fori_loop(0, CH // 32, steps, state[...])

        @pl.when(c == 0)
        def _():
            g_wo.stage4()

        rows = pl.ds(base, CH)
        for target in range(SIDE):
            for side, ref in ((core, keep1), (1 - core, give1)):
                ref[target, rows, :] = jnp.dot(
                    carried[...], wo[target, side], preferred_element_type=F32
                ).astype(BF16)
        sum1.stage0(c)

    def settle(c):
        rows = pl.ds(pl.multiple_of(c * CH, CH), CH)
        full2[tp, rows, :] = (full1[tp, rows, :].astype(F32) + sum1.stage3(c)).astype(BF16)
        spread2.stage0(c)

    def feed(c):
        spread2.stage3(c)
        norm_chunk(full2, gain2, nrm, c)
        ffo[...] = jnp.dot(nrm[...], wff[...].reshape(2048, 2 * FFL), preferred_element_type=F32)

        def act(i, carry):
            rows = pl.ds(pl.multiple_of(i * 16, 16), 16)
            hid[rows, :GU] = (jax.nn.silu(ffo[rows, :GU]) * ffo[rows, GU : 2 * GU]).astype(BF16)
            tail = ffo[rows, 2 * GU :]
            hid[rows, GU:] = (jax.nn.silu(tail[:, :64]) * tail[:, 64:]).astype(BF16)
            return carry

        lax.fori_loop(0, CH // 16, act, 0, unroll=2)

        @pl.when(c == 0)
        def _():
            g_wd.stage4()

        rows = pl.ds(pl.multiple_of(c * CH, CH), CH)
        for target in range(SIDE):
            for side, ref in ((core, keep2), (1 - core, give2)):
                ref[target, rows, :] = jnp.dot(
                    hid[...], wd[target, side], preferred_element_type=F32
                ).astype(BF16)
        sum2.stage0(c)

    def finish(c):
        rows = pl.ds(pl.multiple_of(c * CH, CH), CH)
        out[rows, :] = (full2[tp, rows, :].astype(F32) + sum2.stage3(c)).astype(BF16)

    stages = [
        (9, sum2.stage2),
        (8, sum2.stage1),
        (5, spread2.stage2),
        (4, spread2.stage1),
        (3, settle),
        (2, sum1.stage2),
        (1, sum1.stage1),
        (0, mix),
        (7, feed),
        (10, finish),
    ]

    def tick(i, carry):
        @pl.when(i == 4)
        def _():
            g_wff.stage3()

        @pl.when(i == 6)
        def _():
            g_wd.stage3()

        @pl.when(i == 7)
        def _():
            g_wff.stage4()

        for lag, stage in stages:
            pl.when((i >= lag) & (i < lag + CHUNKS))(functools.partial(stage, i - lag))
        return carry

    lax.fori_loop(0, CHUNKS + 10, tick, 0)

    for gather in gathers:
        gather.drain()

    def drained(c, carry):
        for group in (spread1, spread2, sum1, sum2):
            group.drain(c)
        return carry

    lax.fori_loop(0, CHUNKS, drained, 0)


def layer(tok, wgi, wo, wff, wd, gm, small, ld, gain1, gain2):
    anywhere = pl.BlockSpec(memory_space=pl.ANY)
    vmem = pl.BlockSpec(memory_space=pltpu.VMEM)
    sums = [
        pltpu.VMEM((SIDE, ROWS, CB), BF16),
        pltpu.VMEM((SIDE, ROWS, CB), BF16),
        pltpu.VMEM((SIDE, ROWS, CB), BF16),
        pltpu.VMEM((SIDE, ROWS, CB), BF16),
        pltpu.VMEM((2, CHUNKS, HALF, CB), BF16),
        pltpu.VMEM((2, ROWS, CB), BF16),
    ]
    return pl.pallas_call(
        kernel,
        out_shape=jax.ShapeDtypeStruct((ROWS, CB), BF16),
        in_specs=[anywhere] * 5 + [vmem] * 5,
        out_specs=vmem,
        scratch_shapes=[
            pltpu.VMEM((8, ROWS, CB), BF16),
            pltpu.VMEM((8, ROWS, CB), BF16),
            pltpu.VMEM((SIDE, SIDE, 128, 2 * RP), BF16),
            pltpu.VMEM((SIDE, 2, RP, CB), BF16),
            pltpu.VMEM((SIDE, SIDE, 128, 2 * FFL), BF16),
            pltpu.VMEM((SIDE, 2, FFL, CB), BF16),
            *sums,
            *sums,
            pltpu.VMEM((24 + ROWS, RP), F32),
            pltpu.VMEM((CH, RP), F32),
            pltpu.VMEM((CH, RP), BF16),
            pltpu.VMEM((CH, 2 * RP), F32),
            pltpu.VMEM((CH, RP), BF16),
            pltpu.VMEM((CH, 2048), BF16),
            pltpu.VMEM((CH, 2 * FFL), F32),
            pltpu.VMEM((CH, FFL), BF16),
            pltpu.VMEM((SEQS, RP), F32),
            pltpu.SemaphoreType.DMA((5,)),
            pltpu.SemaphoreType.DMA((4, 2, 8)),
            pltpu.SemaphoreType.DMA((4, 2, 8)),
            pltpu.SemaphoreType.DMA((2, 8, CHUNKS)),
            pltpu.SemaphoreType.DMA((2, 8, CHUNKS)),
            pltpu.SemaphoreType.DMA((2, 5, CHUNKS)),
            pltpu.SemaphoreType.DMA((2, 5, CHUNKS)),
        ],
        compiler_params=pltpu.CompilerParams(
            collective_id=0, has_side_effects=True, vmem_limit_bytes=66_000_000
        ),
    )(tok, wgi, wo, wff, wd, gm, small, ld, gain1, gain2)


def shards(
    tokens,
    recurrence_norm_gain,
    output_gate_weight,
    recurrence_input_weight,
    convolution_taps,
    recurrence_gate_weight,
    input_gate_weight,
    base_decay_logit,
    token_log_decay,
    recurrence_output_weight,
    feedforward_norm_gain,
    feedforward_gate_weight,
    feedforward_up_weight,
    feedforward_down_weight,
):
    tok = tokens.reshape(SEQS, LEN, CB).transpose(1, 0, 2).reshape(ROWS, CB)
    ld = token_log_decay.reshape(SEQS, LEN).T.reshape(ROWS, 1)
    pad = ((0, 0), (0, RP - 352))
    wgi = jnp.concatenate([jnp.pad(output_gate_weight, pad), jnp.pad(recurrence_input_weight, pad)], axis=1)
    square = ((0, RP - 352), (0, RP - 352))
    gm = jnp.concatenate(
        [jnp.pad(recurrence_gate_weight[0], square), jnp.pad(input_gate_weight[0], square)], axis=1
    )
    wff = jnp.concatenate(
        [
            feedforward_gate_weight[:, :GU],
            feedforward_up_weight[:, :GU],
            feedforward_gate_weight[:, GU:],
            feedforward_up_weight[:, GU:],
        ],
        axis=1,
    )
    rate = -GATE_EXPONENT * jax.nn.softplus(-base_decay_logit)
    small = jnp.pad(jnp.concatenate([convolution_taps, rate[None, :]], axis=0), ((0, 3), (0, RP - 352)))
    out = layer(
        tok,
        wgi,
        recurrence_output_weight,
        wff,
        feedforward_down_weight,
        gm,
        small,
        ld,
        recurrence_norm_gain.reshape(8, CB),
        feedforward_norm_gain.reshape(8, CB),
    )
    return out.reshape(LEN, SEQS, CB).transpose(1, 0, 2).reshape(ROWS, CB)


def solution(mesh):
    in_specs = (
        P("fs", "tp"),
        P(),
        P("fs", "tp"),
        P("fs", "tp"),
        P(None, "tp"),
        P("tp", None, None),
        P("tp", None, None),
        P("tp"),
        P("fs"),
        P("tp", "fs"),
        P(),
        P("fs", "tp"),
        P("fs", "tp"),
        P("tp", "fs"),
    )
    return jax.shard_map(shards, mesh=mesh, in_specs=in_specs, out_specs=P("fs", "tp"), check_vma=False)
```

```python
import functools

import jax
import jax.numpy as jnp
from jax import lax
from jax.experimental import pallas as pl
from jax.experimental.pallas import tpu as pltpu
from jax.sharding import PartitionSpec as P

MESH = pl.DeviceIdType.MESH
F32 = jnp.float32
BF16 = jnp.bfloat16

LEN = 128
EPSILON = 1e-06
GATE_EXPONENT = 8.0

SIDE = 4
CHUNKS = 4
ROWS = 1024
CH = ROWS // CHUNKS
HALF = CH // 2
STEPS = LEN // CHUNKS
SEQS = 8
R = 352
RP = 384
FFL = 704
FP = 768
CB = 256
NT = (((1,), (1,)), ((), ()))

WGI_ROWS = (((0, 176), (176, 176)), ((RP, 176), (RP + 176, 176)))
WO_ROWS = (((0, 96), (96, 80)), ((176, 96), (272, 80)))
WFF_ROWS = (((0, 352), (352, 352)), ((FP, 352), (FP + 352, 352)))
WD_ROWS = (((0, 176), (176, 176)), ((352, 176), (528, 176)))


class Gather:
    def __init__(self, buf, rows, send, recv, pos, dev):
        self.buf, self.rows, self.send, self.recv, self.dev = buf, rows, send, recv, dev
        self.axes = (("x", "z"), ("z", "x"))
        self.pos = pos

    def block(self, part, i1, i2, half=None):
        z, x = (i2, i1) if part == 0 else (i1, i2)
        lo, hi = self.rows[part]
        span = pl.ds(lo[0], lo[1] + hi[1]) if half is None else pl.ds(*(lo, hi)[half])
        return self.buf.at[span, pl.ds(pl.multiple_of((z * SIDE + x) * 128, 128), 128)]

    def copy(self, view, part, k, to):
        return pltpu.make_async_remote_copy(
            src_ref=view,
            dst_ref=view,
            send_sem=self.send.at[part, k],
            recv_sem=self.recv.at[part, k],
            device_id=to,
            device_id_type=MESH,
        )

    def places(self, part):
        a1, a2 = self.axes[part]
        (m1, i1, p1), (m2, i2, p2) = self.pos[a1], self.pos[a2]
        far1, far2 = lax.rem(i1 + 2, SIDE), lax.rem(i2 + 2, SIDE)
        return (i1, m1, p1, far1), (i2, m2, p2, far2), self.dev[a1], self.dev[a2]

    def landing(self, part, k):
        first, second, _, _ = self.places(part)
        if k < 4:
            where = (first[1], first[2], first[3], first[3])[k]
            return self.block(part, where, second[0], None if k < 2 else k - 2)
        q, k = divmod(k - 4, 4)
        where = (second[1], second[2], second[3], second[3])[k]
        return self.block(part, first[q], where, None if k < 2 else k - 2)

    def arrived(self, part, k):
        self.copy(self.landing(part, k), part, k, self.dev["x"][0]).wait_recv()

    def onto_second(self, part, q):
        first, second, _, dev2 = self.places(part)
        view = self.block(part, first[q], second[0])
        self.copy(view, part, 4 + 4 * q, dev2[1]).start()
        self.copy(view, part, 5 + 4 * q, dev2[0]).start()

    def own(self):
        for part in (0, 1):
            first, second, dev1, _ = self.places(part)
            view = self.block(part, first[0], second[0])
            self.copy(view, part, 0, dev1[1]).start()
            self.copy(view, part, 1, dev1[0]).start()
        for part in (0, 1):
            self.onto_second(part, 0)

    def near(self):
        for part in (0, 1):
            first, second, dev1, _ = self.places(part)
            self.arrived(part, 0)
            self.copy(self.block(part, first[1], second[0], 0), part, 2, dev1[1]).start()
            self.arrived(part, 1)
            self.copy(self.block(part, first[2], second[0], 1), part, 3, dev1[0]).start()
        for part in (0, 1):
            self.onto_second(part, 1)
            self.onto_second(part, 2)

    def far(self):
        for part in (0, 1):
            self.arrived(part, 2)
            self.arrived(part, 3)
            self.onto_second(part, 3)

    def relay(self, q):
        for part in (0, 1):
            first, second, _, dev2 = self.places(part)
            self.arrived(part, 4 + 4 * q)
            self.copy(self.block(part, first[q], second[1], 0), part, 6 + 4 * q, dev2[1]).start()
            self.arrived(part, 5 + 4 * q)
            self.copy(self.block(part, first[q], second[2], 1), part, 7 + 4 * q, dev2[0]).start()

    def done(self):
        for part in (0, 1):
            for q in range(4):
                self.arrived(part, 6 + 4 * q)
                self.arrived(part, 7 + 4 * q)

    def drain(self):
        for part in (0, 1):
            for k in range(20):
                self.copy(self.landing(part, k), part, k, self.dev["x"][0]).wait_send()


class Spread:
    def __init__(self, buf, send, recv, y, core, dev):
        self.buf, self.send, self.recv, self.dev = buf, send, recv, dev
        (ym, yy, yp), far = y, lax.rem(y[1] + 2, SIDE)
        other = 1 - core
        self.own, self.minus, self.plus, self.far = (2 * v + core for v in (yy, ym, yp, far))
        self.others = [2 * v + other for v in (yy, ym, yp, far)]

    def view(self, block, c, half=None):
        if half is None:
            return self.buf.at[block, pl.ds(pl.multiple_of(c * CH, CH), CH), :]
        return self.buf.at[block, pl.ds(pl.multiple_of(c * CH + half * HALF, HALF), HALF), :]

    def copy(self, view, k, c, to):
        return pltpu.make_async_remote_copy(
            src_ref=view,
            dst_ref=view,
            send_sem=self.send.at[k, c],
            recv_sem=self.recv.at[k, c],
            device_id=to,
            device_id_type=MESH,
        )

    def landing(self, k, c):
        return [
            (self.minus, None),
            (self.plus, None),
            (self.others[0], None),
            (self.far, 0),
            (self.far, 1),
            (self.others[1], None),
            (self.others[2], None),
            (self.others[3], None),
        ][k]

    def arrived(self, k, c):
        block, half = self.landing(k, c)
        self.copy(self.view(block, c, half), k, c, self.dev["core"]).wait_recv()

    def stage0(self, c):
        view = self.view(self.own, c)
        self.copy(view, 0, c, self.dev["y"][1]).start()
        self.copy(view, 1, c, self.dev["y"][0]).start()
        self.copy(view, 2, c, self.dev["core"]).start()

    def stage1(self, c):
        self.arrived(0, c)
        self.copy(self.view(self.minus, c, 0), 3, c, self.dev["y"][1]).start()
        self.copy(self.view(self.minus, c), 5, c, self.dev["core"]).start()
        self.arrived(1, c)
        self.copy(self.view(self.plus, c, 1), 4, c, self.dev["y"][0]).start()
        self.copy(self.view(self.plus, c), 6, c, self.dev["core"]).start()

    def stage2(self, c):
        self.arrived(3, c)
        self.arrived(4, c)
        self.copy(self.view(self.far, c), 7, c, self.dev["core"]).start()

    def stage3(self, c):
        for k in (2, 5, 6, 7):
            self.arrived(k, c)

    def drain(self, c):
        for k in range(8):
            block, half = self.landing(k, c)
            self.copy(self.view(block, c, half), k, c, self.dev["core"]).wait_send()


class Sum:
    def __init__(self, part, took, total, halves, finals, send, recv, y, core, dev):
        self.part, self.took, self.total = part, took, total
        self.halves, self.finals, self.send, self.recv, self.dev = halves, finals, send, recv, dev
        self.minus, self.own, self.plus = y
        self.far = lax.rem(y[1] + 2, SIDE)
        self.core = core

    def rows(self, c):
        return pl.ds(pl.multiple_of(c * CH, CH), CH)

    def half(self, c, h):
        return pl.ds(pl.multiple_of(c * CH + h * HALF, HALF), HALF)

    def parts(self, k, c):
        if k == 0:
            return self.part.at[:, 1 - self.core, self.rows(c), :], self.took.at[:, self.rows(c), :], self.dev["core"]
        if k <= 2:
            return self.total.at[self.far, self.half(c, k - 1), :], self.halves.at[k - 1, c], self.dev["y"][2 - k]
        to = self.plus if k == 3 else self.minus
        return self.total.at[to, self.rows(c), :], self.finals.at[k - 3, self.rows(c), :], self.dev["y"][4 - k]

    def copy(self, k, c):
        src, dst, to = self.parts(k, c)
        return pltpu.make_async_remote_copy(
            src_ref=src,
            dst_ref=dst,
            send_sem=self.send.at[k, c],
            recv_sem=self.recv.at[k, c],
            device_id=to,
            device_id_type=MESH,
        )

    def stage0(self, c):
        self.copy(0, c).start()

    def stage1(self, c):
        self.copy(0, c).wait_recv()
        rows = self.rows(c)

        def add(target):
            self.total[target, rows, :] = (
                self.part[target, self.core, rows, :].astype(F32) + self.took[target, rows, :].astype(F32)
            ).astype(BF16)

        add(self.far)
        add(self.plus)
        self.copy(1, c).start()
        self.copy(2, c).start()
        add(self.minus)
        add(self.own)

    def stage2(self, c):
        for h, target in ((0, self.plus), (1, self.minus)):
            self.copy(1 + h, c).wait_recv()
            rows = self.half(c, h)
            self.total[target, rows, :] = (
                self.total[target, rows, :].astype(F32) + self.halves[h, c].astype(F32)
            ).astype(BF16)
        self.copy(3, c).start()
        self.copy(4, c).start()

    def stage3(self, c):
        self.copy(3, c).wait_recv()
        self.copy(4, c).wait_recv()
        rows = self.rows(c)
        return (
            self.total[self.own, rows, :].astype(F32)
            + self.finals[0, rows, :].astype(F32)
            + self.finals[1, rows, :].astype(F32)
        )

    def drain(self, c):
        for k in range(5):
            self.copy(k, c).wait_send()


def norm_chunk(full, gain, out, c):
    step = 16

    def body(i, carry):
        rows = pl.ds(pl.multiple_of(c * CH + i * step, step), step)
        here = pl.ds(pl.multiple_of(i * step, step), step)
        total = jnp.zeros((step, CB), F32)
        for b in range(8):
            v = full[b, rows, :].astype(F32)
            total = total + v * v
        scale = lax.rsqrt(jnp.sum(total, axis=1, keepdims=True) * (1.0 / 2048.0) + EPSILON)
        for b in range(8):
            v = full[b, rows, :].astype(F32) * scale
            for s in range(2):
                g = gain[2 * b + s : 2 * b + s + 1, :]
                lo = b * CB + s * 128
                out[here, lo : lo + 128] = (v[:, s * 128 : s * 128 + 128] * g).astype(BF16)
        return carry

    lax.fori_loop(0, CH // step, body, 0, unroll=2)


def order(shape, major):
    to = lax.broadcasted_iota(jnp.int32, shape, 0)
    source = lax.broadcasted_iota(jnp.int32, shape, 1)
    if major == "time":
        wanted = lax.rem(to, SEQS) * STEPS + to // SEQS
    else:
        wanted = lax.rem(to, STEPS) * SEQS + to // STEPS
    return jnp.where(source == wanted, 1.0, 0.0).astype(BF16)


def kernel(
    wg_hbm, wi_hbm, tok_hbm, wo_hbm, wfg_hbm, wfu_hbm, wd_hbm,
    gr_hbm, gi_hbm, taps_hbm, base_hbm, ld_hbm, gain1_hbm, gain2_hbm,
    out,
    full1, full2, wgi, wo, wff, wd,
    part1, took1, total1, halves1, finals1,
    part2, took2, total2, halves2, finals2,
    tokv, grv, giv, tapsv, basev, ldv, gain1, gain2,
    gm, small, ldb, perm,
    feat, proj, mixed, gl, carried, nrm, ffo, hid, state,
    local_sem, w_send, w_recv, a_send, a_recv, s_send, s_recv,
):
    fs, tp = lax.axis_index("fs"), lax.axis_index("tp")
    iz, ix = fs // SIDE, lax.rem(fs, SIDE)
    iy, core = tp // 2, lax.rem(tp, 2)

    def ring(i):
        return lax.rem(i + SIDE - 1, SIDE), i, lax.rem(i + 1, SIDE)

    pos = {"x": ring(ix), "z": ring(iz)}
    y = ring(iy)
    dev = {
        "x": tuple({"fs": iz * SIDE + pos["x"][k]} for k in (0, 2)),
        "z": tuple({"fs": pos["z"][k] * SIDE + ix} for k in (0, 2)),
        "y": tuple({"tp": 2 * y[k] + core} for k in (0, 2)),
        "core": {"tp": 2 * iy + 1 - core},
    }

    barrier = pltpu.get_barrier_semaphore()
    for to in (*dev["x"], *dev["z"], *dev["y"], dev["core"]):
        pl.semaphore_signal(barrier, inc=1, device_id=to, device_id_type=MESH)

    cols = pl.ds(pl.multiple_of(fs * 128, 128), 128)
    local = [
        pltpu.make_async_copy(src, dst, local_sem.at[n])
        for n, (src, dst) in enumerate(
            (
                (wg_hbm, wgi.at[pl.ds(0, R), cols]),
                (wi_hbm, wgi.at[pl.ds(RP, R), cols]),
                (tok_hbm, tokv),
                (wo_hbm, wo.at[pl.ds(0, R), cols]),
                (wfg_hbm, wff.at[pl.ds(0, FFL), cols]),
                (wfu_hbm, wff.at[pl.ds(FP, FFL), cols]),
                (wd_hbm, wd.at[:, cols]),
                (gr_hbm, grv),
                (gi_hbm, giv),
                (taps_hbm, tapsv),
                (base_hbm, basev),
                (ld_hbm, ldv),
                (gain1_hbm, gain1),
                (gain2_hbm, gain2),
            )
        )
    ]
    for copy in local:
        copy.start()
    wgi[R:RP, :] = jnp.zeros((RP - R, 2048), BF16)
    wgi[RP + R :, :] = jnp.zeros((RP - R, 2048), BF16)
    wo[R:RP, :] = jnp.zeros((RP - R, 2048), BF16)
    wff[FFL:FP, :] = jnp.zeros((FP - FFL, 2048), BF16)
    perm[...] = order((CH, CH), "time")

    gathers = [
        Gather(buf, rows, w_send.at[m], w_recv.at[m], pos, dev)
        for m, (buf, rows) in enumerate(((wgi, WGI_ROWS), (wo, WO_ROWS), (wff, WFF_ROWS), (wd, WD_ROWS)))
    ]
    g_wgi, g_wo, g_wff, g_wd = gathers
    spread1 = Spread(full1, a_send.at[0], a_recv.at[0], y, core, dev)
    spread2 = Spread(full2, a_send.at[1], a_recv.at[1], y, core, dev)
    sum1 = Sum(part1, took1, total1, halves1, finals1, s_send.at[0], s_recv.at[0], y, core, dev)
    sum2 = Sum(part2, took2, total2, halves2, finals2, s_send.at[1], s_recv.at[1], y, core, dev)

    def reordered(c):
        pieces = [tokv[s * LEN + c * STEPS : s * LEN + (c + 1) * STEPS, :] for s in range(SEQS)]
        full1[tp, c * CH : (c + 1) * CH, :] = jnp.dot(
            perm[...], jnp.concatenate(pieces, axis=0), preferred_element_type=F32
        ).astype(BF16)

    local[2].wait()
    for c in range(CHUNKS):
        reordered(c)
    local[0].wait()
    local[1].wait()
    pl.semaphore_wait(barrier, 7)

    g_wgi.own()
    for c in range(CHUNKS):
        spread1.stage0(c)
    local[3].wait()
    g_wo.own()

    for n in range(7, 14):
        local[n].wait()
    gm[...] = jnp.zeros_like(gm)
    gm[0:R, 0:R] = grv[...]
    gm[0:R, RP : RP + R] = giv[...]
    small[...] = jnp.zeros_like(small)
    small[0:4, 0:R] = tapsv[...]
    small[4:5, 0:R] = -GATE_EXPONENT * jax.nn.softplus(-basev[...])
    for t in range(LEN):
        ldb[8 * t : 8 * t + 8, :] = jnp.broadcast_to(ldv[:, t : t + 1], (SEQS, 128))
    feat[0:24, :] = jnp.zeros((24, RP), F32)
    state[...] = jnp.zeros_like(state)
    for n in range(4, 7):
        local[n].wait()

    g_wgi.near()
    spread1.stage1(0)
    g_wgi.relay(0)
    g_wo.near()
    spread1.stage1(1)
    g_wgi.far()
    g_wgi.relay(1)
    spread1.stage1(2)
    g_wo.relay(0)
    g_wgi.relay(2)
    g_wo.far()
    spread1.stage1(3)
    spread1.stage2(0)
    g_wo.relay(1)
    spread1.stage2(1)
    g_wgi.relay(3)
    g_wo.relay(2)
    g_wo.relay(3)
    g_wff.own()
    spread1.stage2(2)
    spread1.stage2(3)

    def mix_in(c):
        spread1.stage3(c)
        norm_chunk(full1, gain1, nrm, c)
        base = pl.multiple_of(c * CH, CH)

        @pl.when(c == 0)
        def _():
            g_wgi.done()

        projected = lax.dot_general(nrm[...], wgi[...], NT, preferred_element_type=F32)
        proj[...] = projected[:, :RP]
        feat[pl.ds(base + 24, CH), :] = projected[:, RP:].astype(BF16).astype(F32)

    def mix_out(c):
        base = pl.multiple_of(c * CH, CH)

        def taps(i, carry):
            r = pl.multiple_of(i * 32, 32)
            summed = small[0:1, :] * feat[pl.ds(base + r, 32), :]
            for k in range(1, 4):
                summed = summed + small[k : k + 1, :] * feat[pl.ds(base + r + 8 * k, 32), :]
            mixed[pl.ds(r, 32), :] = summed.astype(BF16)
            return carry

        lax.fori_loop(0, CH // 32, taps, 0, unroll=2)
        gl[...] = jnp.dot(mixed[...], gm[...], preferred_element_type=F32)

        def steps(i, h):
            r = pl.multiple_of(i * 32, 32)
            rows = pl.ds(r, 32)
            recur = jax.nn.sigmoid(gl[rows, :RP])
            inject = jax.nn.sigmoid(gl[rows, RP:])
            struck = ldb[pl.ds(base + r, 32), :]
            log_decay = small[4:5, :] * recur + jnp.concatenate([struck] * 3, axis=1)
            decay = jnp.exp(log_decay)
            twice = 2.0 * log_decay
            near = -twice * (1.0 + twice * (0.5 + twice * (1.0 / 6.0 + twice * (1.0 / 24.0 + twice * (1.0 / 120.0)))))
            rest = jnp.where(twice > -0.1, near, 1.0 - decay * decay)
            driven = jnp.sqrt(rest) * (inject * mixed[rows, :].astype(F32))
            states = []
            for s in range(4):
                h = decay[8 * s : 8 * s + 8] * h + driven[8 * s : 8 * s + 8]
                states.append(h)
            carried[rows, :] = (jnp.concatenate(states, axis=0) * jax.nn.gelu(proj[rows, :])).astype(BF16)
            return h

        state[...] = lax.fori_loop(0, CH // 32, steps, state[...])

        @pl.when(c == 0)
        def _():
            g_wo.done()

        rows = pl.ds(base, CH)
        for j in range(8):
            part1[j // 2, j % 2, rows, :] = jnp.dot(
                carried[...], wo[:, j * CB : (j + 1) * CB], preferred_element_type=F32
            ).astype(BF16)
        sum1.stage0(c)

    def settle(c):
        rows = pl.ds(pl.multiple_of(c * CH, CH), CH)
        full2[tp, rows, :] = (full1[tp, rows, :].astype(F32) + sum1.stage3(c)).astype(BF16)
        spread2.stage0(c)

    def up(c):
        spread2.stage3(c)
        norm_chunk(full2, gain2, nrm, c)

        @pl.when(c == 0)
        def _():
            g_wff.done()

        ffo[...] = lax.dot_general(nrm[...], wff[...], NT, preferred_element_type=F32)
        base = pl.multiple_of(c * CH, CH)

        def act(i, carry):
            r = pl.multiple_of(i * 16, 16)
            rows = pl.ds(r, 16)
            hid[pl.ds(base + r, 16), :] = (jax.nn.silu(ffo[rows, :FFL]) * ffo[rows, FP:]).astype(BF16)
            return carry

        lax.fori_loop(0, CH // 16, act, 0, unroll=2)

    def down(c):
        @pl.when(c == 0)
        def _():
            g_wd.done()

        rows = pl.ds(pl.multiple_of(c * CH, CH), CH)
        for j in range(8):
            part2[j // 2, j % 2, rows, :] = jnp.dot(
                hid[rows, :], wd[:, j * CB : (j + 1) * CB], preferred_element_type=F32
            ).astype(BF16)
        sum2.stage0(c)

    def finish(c):
        rows = pl.ds(pl.multiple_of(c * CH, CH), CH)
        layer_out = (full2[tp, rows, :].astype(F32) + sum2.stage3(c)).astype(BF16)
        ordered = jnp.dot(perm[...], layer_out, preferred_element_type=F32).astype(BF16)
        for s in range(SEQS):
            out[pl.ds(pl.multiple_of(s * LEN + c * STEPS, STEPS), STEPS), :] = ordered[s * STEPS : (s + 1) * STEPS]

    def turn(c):
        @pl.when(c == 0)
        def _():
            perm[...] = order((CH, CH), "sequence")

    events = {
        0: (g_wff.near,),
        1: (functools.partial(g_wff.relay, 0), g_wff.far),
        2: (functools.partial(g_wff.relay, 1), g_wd.own),
        3: (functools.partial(g_wff.relay, 2),),
        4: (functools.partial(g_wff.relay, 3),),
        5: (g_wd.near,),
        6: (functools.partial(g_wd.relay, 0),),
        7: (g_wd.far,),
        8: (functools.partial(g_wd.relay, 1),),
        9: (functools.partial(g_wd.relay, 2), functools.partial(g_wd.relay, 3)),
    }

    def weights(i):
        for when, calls in events.items():

            @pl.when(i == when)
            def _():
                for call in calls:
                    call()

    stages = [
        (0, mix_in),
        (1, sum1.stage1),
        (2, sum1.stage2),
        (3, settle),
        (0, mix_out),
        (4, spread2.stage1),
        (5, spread2.stage2),
        (None, weights),
        (4, turn),
        (6, up),
        (11, sum2.stage1),
        (10, down),
        (14, sum2.stage2),
        (16, finish),
    ]

    def tick(i, carry):
        for lag, stage in stages:
            if lag is None:
                stage(i)
            else:
                pl.when((i >= lag) & (i < lag + CHUNKS))(functools.partial(stage, i - lag))
        return carry

    lax.fori_loop(0, CHUNKS + 16, tick, 0)

    for gather in gathers:
        gather.drain()

    def drained(c, carry):
        for group in (spread1, spread2, sum1, sum2):
            group.drain(c)
        return carry

    lax.fori_loop(0, CHUNKS, drained, 0)


def layer(*operands):
    sums = [
        pltpu.VMEM((SIDE, 2, ROWS, CB), BF16),
        pltpu.VMEM((SIDE, ROWS, CB), BF16),
        pltpu.VMEM((SIDE, ROWS, CB), BF16),
        pltpu.VMEM((2, CHUNKS, HALF, CB), BF16),
        pltpu.VMEM((2, ROWS, CB), BF16),
    ]
    return pl.pallas_call(
        kernel,
        out_shape=jax.ShapeDtypeStruct((ROWS, CB), BF16),
        in_specs=[pl.BlockSpec(memory_space=pl.ANY)] * len(operands),
        out_specs=pl.BlockSpec(memory_space=pltpu.VMEM),
        scratch_shapes=[
            pltpu.VMEM((8, ROWS, CB), BF16),
            pltpu.VMEM((8, ROWS, CB), BF16),
            pltpu.VMEM((2 * RP, 2048), BF16),
            pltpu.VMEM((RP, 2048), BF16),
            pltpu.VMEM((FP + FFL, 2048), BF16),
            pltpu.VMEM((FFL, 2048), BF16),
            *sums,
            *sums,
            pltpu.VMEM((ROWS, CB), BF16),
            pltpu.VMEM((R, R), BF16),
            pltpu.VMEM((R, R), BF16),
            pltpu.VMEM((4, R), F32),
            pltpu.VMEM((1, R), F32),
            pltpu.VMEM((SEQS, LEN), F32),
            pltpu.VMEM((16, 128), F32),
            pltpu.VMEM((16, 128), F32),
            pltpu.VMEM((RP, 2 * RP), BF16),
            pltpu.VMEM((8, RP), F32),
            pltpu.VMEM((ROWS, 128), F32),
            pltpu.VMEM((CH, CH), BF16),
            pltpu.VMEM((24 + ROWS, RP), F32),
            pltpu.VMEM((CH, RP), F32),
            pltpu.VMEM((CH, RP), BF16),
            pltpu.VMEM((CH, 2 * RP), F32),
            pltpu.VMEM((CH, RP), BF16),
            pltpu.VMEM((CH, 2048), BF16),
            pltpu.VMEM((CH, FP + FFL), F32),
            pltpu.VMEM((ROWS, FFL), BF16),
            pltpu.VMEM((SEQS, RP), F32),
            pltpu.SemaphoreType.DMA((14,)),
            pltpu.SemaphoreType.DMA((4, 2, 20)),
            pltpu.SemaphoreType.DMA((4, 2, 20)),
            pltpu.SemaphoreType.DMA((2, 8, CHUNKS)),
            pltpu.SemaphoreType.DMA((2, 8, CHUNKS)),
            pltpu.SemaphoreType.DMA((2, 5, CHUNKS)),
            pltpu.SemaphoreType.DMA((2, 5, CHUNKS)),
        ],
        compiler_params=pltpu.CompilerParams(
            collective_id=0, has_side_effects=True, vmem_limit_bytes=66_000_000
        ),
    )(*operands)


def shards(
    tokens,
    recurrence_norm_gain,
    output_gate_weight,
    recurrence_input_weight,
    convolution_taps,
    recurrence_gate_weight,
    input_gate_weight,
    base_decay_logit,
    token_log_decay,
    recurrence_output_weight,
    feedforward_norm_gain,
    feedforward_gate_weight,
    feedforward_up_weight,
    feedforward_down_weight,
):
    return layer(
        output_gate_weight.T,
        recurrence_input_weight.T,
        tokens,
        recurrence_output_weight,
        feedforward_gate_weight.T,
        feedforward_up_weight.T,
        feedforward_down_weight,
        recurrence_gate_weight.reshape(R, R),
        input_gate_weight.reshape(R, R),
        convolution_taps,
        base_decay_logit.reshape(1, R),
        token_log_decay.reshape(SEQS, LEN),
        recurrence_norm_gain.reshape(16, 128),
        feedforward_norm_gain.reshape(16, 128),
    )


def solution(mesh):
    in_specs = (
        P("fs", "tp"),
        P(),
        P("fs", "tp"),
        P("fs", "tp"),
        P(None, "tp"),
        P("tp", None, None),
        P("tp", None, None),
        P("tp"),
        P("fs"),
        P("tp", "fs"),
        P(),
        P("fs", "tp"),
        P("fs", "tp"),
        P("tp", "fs"),
    )
    return jax.shard_map(shards, mesh=mesh, in_specs=in_specs, out_specs=P("fs", "tp"), check_vma=False)
```

```python
import jax
import jax.numpy as jnp
from jax import lax
from jax.experimental import pallas as pl
from jax.experimental.pallas import tpu as pltpu
from jax.sharding import PartitionSpec as P

MESH = pl.DeviceIdType.MESH
F32 = jnp.float32
BF16 = jnp.bfloat16

LEN = 128
EPSILON = 1e-06
GATE_EXPONENT = 8.0

SIDE = 4
CHUNKS = 4
ROWS = 1024
CH = ROWS // CHUNKS
HALF = CH // 2
STEPS = LEN // CHUNKS
SEQS = 8
R = 352
RP = 384
FFL = 704
FP = 768
CB = 256
NT = (((1,), (1,)), ((), ()))

WGI_ROWS = (((0, 176), (176, 176)), ((RP, 176), (RP + 176, 176)))
WO_ROWS = (((0, 96), (96, 80)), ((176, 96), (272, 80)))
WFF_ROWS = (((0, 352), (352, 352)), ((FP, 352), (FP + 352, 352)))
WD_ROWS = (((0, 176), (176, 176)), ((352, 176), (528, 176)))


class Gather:
    def __init__(self, buf, rows, send, recv, pos, dev):
        self.buf, self.rows, self.send, self.recv, self.dev = buf, rows, send, recv, dev
        self.axes = (("x", "z"), ("z", "x"))
        self.pos = pos

    def block(self, part, i1, i2, half=None):
        z, x = (i2, i1) if part == 0 else (i1, i2)
        lo, hi = self.rows[part]
        span = pl.ds(lo[0], lo[1] + hi[1]) if half is None else pl.ds(*(lo, hi)[half])
        return self.buf.at[span, pl.ds(pl.multiple_of((z * SIDE + x) * 128, 128), 128)]

    def copy(self, view, part, k, to):
        return pltpu.make_async_remote_copy(
            src_ref=view,
            dst_ref=view,
            send_sem=self.send.at[part, k],
            recv_sem=self.recv.at[part, k],
            device_id=to,
            device_id_type=MESH,
        )

    def places(self, part):
        a1, a2 = self.axes[part]
        (m1, i1, p1), (m2, i2, p2) = self.pos[a1], self.pos[a2]
        far1, far2 = lax.rem(i1 + 2, SIDE), lax.rem(i2 + 2, SIDE)
        return (i1, m1, p1, far1), (i2, m2, p2, far2), self.dev[a1], self.dev[a2]

    def landing(self, part, k):
        first, second, _, _ = self.places(part)
        if k < 4:
            where = (first[1], first[2], first[3], first[3])[k]
            return self.block(part, where, second[0], None if k < 2 else k - 2)
        q, k = divmod(k - 4, 4)
        where = (second[1], second[2], second[3], second[3])[k]
        return self.block(part, first[q], where, None if k < 2 else k - 2)

    def arrived(self, part, k):
        self.copy(self.landing(part, k), part, k, self.dev["x"][0]).wait_recv()

    def onto_second(self, part, q):
        first, second, _, dev2 = self.places(part)
        view = self.block(part, first[q], second[0])
        self.copy(view, part, 4 + 4 * q, dev2[1]).start()
        self.copy(view, part, 5 + 4 * q, dev2[0]).start()

    def own(self):
        for part in (0, 1):
            first, second, dev1, _ = self.places(part)
            view = self.block(part, first[0], second[0])
            self.copy(view, part, 0, dev1[1]).start()
            self.copy(view, part, 1, dev1[0]).start()
        for part in (0, 1):
            self.onto_second(part, 0)

    def near(self):
        for part in (0, 1):
            first, second, dev1, _ = self.places(part)
            self.arrived(part, 0)
            self.copy(self.block(part, first[1], second[0], 0), part, 2, dev1[1]).start()
            self.arrived(part, 1)
            self.copy(self.block(part, first[2], second[0], 1), part, 3, dev1[0]).start()
        for part in (0, 1):
            self.onto_second(part, 1)
            self.onto_second(part, 2)

    def far(self):
        for part in (0, 1):
            self.arrived(part, 2)
            self.arrived(part, 3)
            self.onto_second(part, 3)

    def relay(self, q):
        for part in (0, 1):
            first, second, _, dev2 = self.places(part)
            self.arrived(part, 4 + 4 * q)
            self.copy(self.block(part, first[q], second[1], 0), part, 6 + 4 * q, dev2[1]).start()
            self.arrived(part, 5 + 4 * q)
            self.copy(self.block(part, first[q], second[2], 1), part, 7 + 4 * q, dev2[0]).start()

    def done(self):
        for part in (0, 1):
            for q in range(4):
                self.arrived(part, 6 + 4 * q)
                self.arrived(part, 7 + 4 * q)

    def drain(self):
        for part in (0, 1):
            for k in range(20):
                self.copy(self.landing(part, k), part, k, self.dev["x"][0]).wait_send()


class Spread:
    def __init__(self, buf, send, recv, y, core, dev):
        self.buf, self.send, self.recv, self.dev = buf, send, recv, dev
        (ym, yy, yp), far = y, lax.rem(y[1] + 2, SIDE)
        other = 1 - core
        self.own, self.minus, self.plus, self.far = (2 * v + core for v in (yy, ym, yp, far))
        self.others = [2 * v + other for v in (yy, ym, yp, far)]

    def view(self, block, c, half=None):
        if half is None:
            return self.buf.at[block, pl.ds(c * CH, CH), :]
        return self.buf.at[block, pl.ds(c * CH + half * HALF, HALF), :]

    def copy(self, view, k, c, to):
        return pltpu.make_async_remote_copy(
            src_ref=view,
            dst_ref=view,
            send_sem=self.send.at[k, c],
            recv_sem=self.recv.at[k, c],
            device_id=to,
            device_id_type=MESH,
        )

    def landing(self, k, c):
        return [
            (self.minus, None),
            (self.plus, None),
            (self.others[0], None),
            (self.far, 0),
            (self.far, 1),
            (self.others[1], None),
            (self.others[2], None),
            (self.others[3], None),
        ][k]

    def arrived(self, k, c):
        block, half = self.landing(k, c)
        self.copy(self.view(block, c, half), k, c, self.dev["core"]).wait_recv()

    def stage0(self, c):
        view = self.view(self.own, c)
        self.copy(view, 0, c, self.dev["y"][1]).start()
        self.copy(view, 1, c, self.dev["y"][0]).start()
        self.copy(view, 2, c, self.dev["core"]).start()

    def stage1(self, c):
        self.arrived(0, c)
        self.copy(self.view(self.minus, c, 0), 3, c, self.dev["y"][1]).start()
        self.copy(self.view(self.minus, c), 5, c, self.dev["core"]).start()
        self.arrived(1, c)
        self.copy(self.view(self.plus, c, 1), 4, c, self.dev["y"][0]).start()
        self.copy(self.view(self.plus, c), 6, c, self.dev["core"]).start()

    def stage2(self, c):
        self.arrived(3, c)
        self.arrived(4, c)
        self.copy(self.view(self.far, c), 7, c, self.dev["core"]).start()

    def stage3(self, c):
        for k in (2, 5, 6, 7):
            self.arrived(k, c)

    def drain(self, c):
        for k in range(8):
            block, half = self.landing(k, c)
            self.copy(self.view(block, c, half), k, c, self.dev["core"]).wait_send()


class Sum:
    def __init__(self, part, took, total, halves, finals, send, recv, y, core, dev):
        self.part, self.took, self.total = part, took, total
        self.halves, self.finals, self.send, self.recv, self.dev = halves, finals, send, recv, dev
        self.minus, self.own, self.plus = y
        self.far = lax.rem(y[1] + 2, SIDE)
        self.core = core

    def rows(self, c):
        return pl.ds(c * CH, CH)

    def half(self, c, h):
        return pl.ds(c * CH + h * HALF, HALF)

    def parts(self, k, c):
        if k == 0:
            return self.part.at[:, 1 - self.core, self.rows(c), :], self.took.at[:, self.rows(c), :], self.dev["core"]
        if k <= 2:
            return self.total.at[self.far, self.half(c, k - 1), :], self.halves.at[k - 1, c], self.dev["y"][2 - k]
        to = self.plus if k == 3 else self.minus
        return self.total.at[to, self.rows(c), :], self.finals.at[k - 3, self.rows(c), :], self.dev["y"][4 - k]

    def copy(self, k, c):
        src, dst, to = self.parts(k, c)
        return pltpu.make_async_remote_copy(
            src_ref=src,
            dst_ref=dst,
            send_sem=self.send.at[k, c],
            recv_sem=self.recv.at[k, c],
            device_id=to,
            device_id_type=MESH,
        )

    def stage0(self, c):
        self.copy(0, c).start()

    def stage1(self, c):
        self.copy(0, c).wait_recv()
        rows = self.rows(c)

        def add(target):
            self.total[target, rows, :] = (
                self.part[target, self.core, rows, :].astype(F32) + self.took[target, rows, :].astype(F32)
            ).astype(BF16)

        add(self.far)
        add(self.plus)
        self.copy(1, c).start()
        self.copy(2, c).start()
        add(self.minus)
        add(self.own)

    def stage2(self, c):
        for h, target in ((0, self.plus), (1, self.minus)):
            self.copy(1 + h, c).wait_recv()
            rows = self.half(c, h)
            self.total[target, rows, :] = (
                self.total[target, rows, :].astype(F32) + self.halves[h, c].astype(F32)
            ).astype(BF16)
        self.copy(3, c).start()
        self.copy(4, c).start()

    def stage3(self, c):
        self.copy(3, c).wait_recv()
        self.copy(4, c).wait_recv()
        rows = self.rows(c)
        return (
            self.total[self.own, rows, :].astype(F32)
            + self.finals[0, rows, :].astype(F32)
            + self.finals[1, rows, :].astype(F32)
        )

    def drain(self, c):
        for k in range(5):
            self.copy(k, c).wait_send()


def norm_chunk(full, gain, out, c):
    step = 16

    def body(i, carry):
        rows = pl.ds(pl.multiple_of(c * CH + i * step, step), step)
        here = pl.ds(pl.multiple_of(i * step, step), step)
        total = jnp.zeros((step, CB), F32)
        for b in range(8):
            v = full[b, rows, :].astype(F32)
            total = total + v * v
        scale = lax.rsqrt(jnp.sum(total, axis=1, keepdims=True) * (1.0 / 2048.0) + EPSILON)
        for b in range(8):
            v = full[b, rows, :].astype(F32) * scale
            for s in range(2):
                g = gain[2 * b + s : 2 * b + s + 1, :]
                lo = b * CB + s * 128
                out[here, lo : lo + 128] = (v[:, s * 128 : s * 128 + 128] * g).astype(BF16)
        return carry

    lax.fori_loop(0, CH // step, body, 0, unroll=2)


def order(shape, major):
    to = lax.broadcasted_iota(jnp.int32, shape, 0)
    source = lax.broadcasted_iota(jnp.int32, shape, 1)
    if major == "time":
        wanted = lax.rem(to, SEQS) * STEPS + to // SEQS
    else:
        wanted = lax.rem(to, STEPS) * SEQS + to // STEPS
    return jnp.where(source == wanted, 1.0, 0.0).astype(BF16)


def kernel(
    wg_hbm, wi_hbm, tok_hbm, wo_hbm, wfg_hbm, wfu_hbm, wd_hbm,
    gr_hbm, gi_hbm, taps_hbm, base_hbm, ld_hbm, gain1_hbm, gain2_hbm,
    out,
    full1, full2, wgi, wo, wff, wd,
    part1, took1, total1, halves1, finals1,
    part2, took2, total2, halves2, finals2,
    tokv, grv, giv, tapsv, basev, ldv, gain1, gain2,
    gm, small, ldb, perm,
    feat, proj, mixed, gl, carried, nrm, ffo, hid, state,
    local_sem, w_send, w_recv, a_send, a_recv, s_send, s_recv,
):
    fs, tp = lax.axis_index("fs"), lax.axis_index("tp")
    iz, ix = fs // SIDE, lax.rem(fs, SIDE)
    iy, core = tp // 2, lax.rem(tp, 2)

    def ring(i):
        return lax.rem(i + SIDE - 1, SIDE), i, lax.rem(i + 1, SIDE)

    pos = {"x": ring(ix), "z": ring(iz)}
    y = ring(iy)
    dev = {
        "x": tuple({"fs": iz * SIDE + pos["x"][k]} for k in (0, 2)),
        "z": tuple({"fs": pos["z"][k] * SIDE + ix} for k in (0, 2)),
        "y": tuple({"tp": 2 * y[k] + core} for k in (0, 2)),
        "core": {"tp": 2 * iy + 1 - core},
    }

    barrier = pltpu.get_barrier_semaphore()
    for to in (*dev["x"], *dev["z"], *dev["y"], dev["core"]):
        pl.semaphore_signal(barrier, inc=1, device_id=to, device_id_type=MESH)

    cols = pl.ds(pl.multiple_of(fs * 128, 128), 128)
    local = [
        pltpu.make_async_copy(src, dst, local_sem.at[n])
        for n, (src, dst) in enumerate(
            (
                (wg_hbm, wgi.at[pl.ds(0, R), cols]),
                (wi_hbm, wgi.at[pl.ds(RP, R), cols]),
                (tok_hbm, tokv),
                (wo_hbm, wo.at[pl.ds(0, R), cols]),
                (wfg_hbm, wff.at[pl.ds(0, FFL), cols]),
                (wfu_hbm, wff.at[pl.ds(FP, FFL), cols]),
                (wd_hbm, wd.at[:, cols]),
                (gr_hbm, grv),
                (gi_hbm, giv),
                (taps_hbm, tapsv),
                (base_hbm, basev),
                (ld_hbm, ldv),
                (gain1_hbm, gain1),
                (gain2_hbm, gain2),
            )
        )
    ]
    for copy in local:
        copy.start()
    wgi[R:RP, :] = jnp.zeros((RP - R, 2048), BF16)
    wgi[RP + R :, :] = jnp.zeros((RP - R, 2048), BF16)
    wo[R:RP, :] = jnp.zeros((RP - R, 2048), BF16)
    wff[FFL:FP, :] = jnp.zeros((FP - FFL, 2048), BF16)
    perm[...] = order((CH, CH), "time")

    gathers = [
        Gather(buf, rows, w_send.at[m], w_recv.at[m], pos, dev)
        for m, (buf, rows) in enumerate(((wgi, WGI_ROWS), (wo, WO_ROWS), (wff, WFF_ROWS), (wd, WD_ROWS)))
    ]
    g_wgi, g_wo, g_wff, g_wd = gathers
    spread1 = Spread(full1, a_send.at[0], a_recv.at[0], y, core, dev)
    spread2 = Spread(full2, a_send.at[1], a_recv.at[1], y, core, dev)
    sum1 = Sum(part1, took1, total1, halves1, finals1, s_send.at[0], s_recv.at[0], y, core, dev)
    sum2 = Sum(part2, took2, total2, halves2, finals2, s_send.at[1], s_recv.at[1], y, core, dev)

    def reordered(c):
        pieces = [tokv[s * LEN + c * STEPS : s * LEN + (c + 1) * STEPS, :] for s in range(SEQS)]
        full1[tp, c * CH : (c + 1) * CH, :] = jnp.dot(
            perm[...], jnp.concatenate(pieces, axis=0), preferred_element_type=F32
        ).astype(BF16)

    local[2].wait()
    for c in range(CHUNKS):
        reordered(c)
    local[0].wait()
    local[1].wait()
    pl.semaphore_wait(barrier, 7)

    def small_operands():
        for n in range(7, 14):
            local[n].wait()
        gm[...] = jnp.zeros_like(gm)
        gm[0:R, 0:R] = grv[...]
        gm[0:R, RP : RP + R] = giv[...]
        small[...] = jnp.zeros_like(small)
        small[0:4, 0:R] = tapsv[...]
        small[4:5, 0:R] = -GATE_EXPONENT * jax.nn.softplus(-basev[...])
        for t in range(LEN):
            ldb[8 * t : 8 * t + 8, :] = jnp.broadcast_to(ldv[:, t : t + 1], (SEQS, 128))
        feat[0:24, :] = jnp.zeros((24, RP), F32)
        state[...] = jnp.zeros_like(state)

    def norm1(c):
        spread1.stage3(c)
        norm_chunk(full1, gain1, nrm, c)

    def project(c):
        base = c * CH
        projected = lax.dot_general(nrm[...], wgi[...], NT, preferred_element_type=F32)
        proj[...] = projected[:, :RP]
        feat[pl.ds(base + 24, CH), :] = projected[:, RP:].astype(BF16).astype(F32)

    def scan(c):
        base = c * CH

        def taps(i, carry):
            r = pl.multiple_of(i * 32, 32)
            summed = small[0:1, :] * feat[pl.ds(base + r, 32), :]
            for k in range(1, 4):
                summed = summed + small[k : k + 1, :] * feat[pl.ds(base + r + 8 * k, 32), :]
            mixed[pl.ds(r, 32), :] = summed.astype(BF16)
            return carry

        lax.fori_loop(0, CH // 32, taps, 0, unroll=2)
        gl[...] = jnp.dot(mixed[...], gm[...], preferred_element_type=F32)

        def steps(i, h):
            r = pl.multiple_of(i * 32, 32)
            rows = pl.ds(r, 32)
            recur = jax.nn.sigmoid(gl[rows, :RP])
            inject = jax.nn.sigmoid(gl[rows, RP:])
            struck = ldb[pl.ds(base + r, 32), :]
            log_decay = small[4:5, :] * recur + jnp.concatenate([struck] * 3, axis=1)
            decay = jnp.exp(log_decay)
            twice = 2.0 * log_decay
            near = -twice * (1.0 + twice * (0.5 + twice * (1.0 / 6.0 + twice * (1.0 / 24.0 + twice * (1.0 / 120.0)))))
            rest = jnp.where(twice > -0.1, near, 1.0 - decay * decay)
            driven = jnp.sqrt(rest) * (inject * mixed[rows, :].astype(F32))
            states = []
            for s in range(4):
                h = decay[8 * s : 8 * s + 8] * h + driven[8 * s : 8 * s + 8]
                states.append(h)
            carried[rows, :] = (jnp.concatenate(states, axis=0) * jax.nn.gelu(proj[rows, :])).astype(BF16)
            return h

        state[...] = lax.fori_loop(0, CH // 32, steps, state[...])

    def mix_out(c):
        rows = pl.ds(c * CH, CH)
        for j in range(8):
            part1[j // 2, j % 2, rows, :] = jnp.dot(
                carried[...], wo[:, j * CB : (j + 1) * CB], preferred_element_type=F32
            ).astype(BF16)
        sum1.stage0(c)

    def settle(c):
        rows = pl.ds(c * CH, CH)
        full2[tp, rows, :] = (full1[tp, rows, :].astype(F32) + sum1.stage3(c)).astype(BF16)
        spread2.stage0(c)

    def norm2(c):
        spread2.stage3(c)
        norm_chunk(full2, gain2, nrm, c)

    def up(c):
        ffo[...] = lax.dot_general(nrm[...], wff[...], NT, preferred_element_type=F32)

    def act(c):
        base = c * CH

        def body(i, carry):
            r = pl.multiple_of(i * 16, 16)
            rows = pl.ds(r, 16)
            hid[pl.ds(base + r, 16), :] = (jax.nn.silu(ffo[rows, :FFL]) * ffo[rows, FP:]).astype(BF16)
            return carry

        lax.fori_loop(0, CH // 16, body, 0, unroll=2)

    def down(c):
        rows = pl.ds(c * CH, CH)
        for j in range(8):
            part2[j // 2, j % 2, rows, :] = jnp.dot(
                hid[rows, :], wd[:, j * CB : (j + 1) * CB], preferred_element_type=F32
            ).astype(BF16)
        sum2.stage0(c)

    def finish(c):
        rows = pl.ds(c * CH, CH)
        layer_out = (full2[tp, rows, :].astype(F32) + sum2.stage3(c)).astype(BF16)
        ordered = jnp.dot(perm[...], layer_out, preferred_element_type=F32).astype(BF16)
        for s in range(SEQS):
            out[pl.ds(s * LEN + c * STEPS, STEPS), :] = ordered[s * STEPS : (s + 1) * STEPS]

    g_wgi.own()
    spread1.stage0(0)
    local[3].wait()
    g_wo.own()
    spread1.stage0(1)
    spread1.stage0(3)
    spread1.stage0(2)
    small_operands()
    g_wgi.near()
    g_wo.near()
    spread1.stage1(3)
    g_wgi.far()
    spread1.stage1(1)
    g_wgi.relay(2)
    g_wo.far()
    spread1.stage1(2)
    g_wgi.relay(0)
    spread1.stage1(0)
    g_wgi.relay(1)
    spread1.stage2(3)
    g_wgi.relay(3)
    g_wo.relay(3)
    spread1.stage2(2)
    g_wo.relay(2)
    g_wo.relay(0)
    g_wo.relay(1)
    spread1.stage2(1)
    local[4].wait()
    local[5].wait()
    g_wff.own()
    spread1.stage2(0)
    norm1(0)
    g_wgi.done()
    project(0)
    scan(0)
    g_wo.done()
    mix_out(0)
    norm1(1)
    project(1)
    sum1.stage1(0)
    g_wff.near()
    scan(1)
    mix_out(1)
    sum1.stage1(1)
    sum1.stage2(0)
    g_wff.relay(0)
    g_wff.far()
    local[6].wait()
    g_wd.own()
    norm1(2)
    project(2)
    sum1.stage2(1)
    scan(2)
    mix_out(2)
    settle(0)
    norm1(3)
    project(3)
    sum1.stage1(2)
    settle(1)
    g_wff.relay(2)
    scan(3)
    mix_out(3)
    g_wff.relay(1)
    sum1.stage2(2)
    sum1.stage1(3)
    g_wff.relay(3)
    g_wd.near()
    spread2.stage1(0)
    spread2.stage1(1)
    settle(2)
    sum1.stage2(3)
    spread2.stage2(0)
    norm2(0)
    spread2.stage2(1)
    g_wff.done()
    up(0)
    spread2.stage1(2)
    g_wd.far()
    act(0)
    norm2(1)
    g_wd.relay(1)
    up(1)
    g_wd.relay(2)
    settle(3)
    spread2.stage2(2)
    act(1)
    g_wd.relay(0)
    g_wd.relay(3)
    norm2(2)
    up(2)
    act(2)
    spread2.stage1(3)
    g_wd.done()
    down(0)
    down(1)
    down(2)
    sum2.stage1(0)
    sum2.stage1(1)
    sum2.stage1(2)
    spread2.stage2(3)
    sum2.stage2(0)
    norm2(3)
    up(3)
    sum2.stage2(2)
    act(3)
    down(3)
    perm[...] = order((CH, CH), "sequence")
    finish(0)
    sum2.stage1(3)
    sum2.stage2(1)
    finish(2)
    sum2.stage2(3)
    finish(1)
    finish(3)

    for gather in gathers:
        gather.drain()

    for c in range(CHUNKS):
        for group in (spread1, spread2, sum1, sum2):
            group.drain(c)


def layer(*operands):
    sums = [
        pltpu.VMEM((SIDE, 2, ROWS, CB), BF16),
        pltpu.VMEM((SIDE, ROWS, CB), BF16),
        pltpu.VMEM((SIDE, ROWS, CB), BF16),
        pltpu.VMEM((2, CHUNKS, HALF, CB), BF16),
        pltpu.VMEM((2, ROWS, CB), BF16),
    ]
    return pl.pallas_call(
        kernel,
        out_shape=jax.ShapeDtypeStruct((ROWS, CB), BF16),
        in_specs=[pl.BlockSpec(memory_space=pl.ANY)] * len(operands),
        out_specs=pl.BlockSpec(memory_space=pltpu.VMEM),
        scratch_shapes=[
            pltpu.VMEM((8, ROWS, CB), BF16),
            pltpu.VMEM((8, ROWS, CB), BF16),
            pltpu.VMEM((2 * RP, 2048), BF16),
            pltpu.VMEM((RP, 2048), BF16),
            pltpu.VMEM((FP + FFL, 2048), BF16),
            pltpu.VMEM((FFL, 2048), BF16),
            *sums,
            *sums,
            pltpu.VMEM((ROWS, CB), BF16),
            pltpu.VMEM((R, R), BF16),
            pltpu.VMEM((R, R), BF16),
            pltpu.VMEM((4, R), F32),
            pltpu.VMEM((1, R), F32),
            pltpu.VMEM((SEQS, LEN), F32),
            pltpu.VMEM((16, 128), F32),
            pltpu.VMEM((16, 128), F32),
            pltpu.VMEM((RP, 2 * RP), BF16),
            pltpu.VMEM((8, RP), F32),
            pltpu.VMEM((ROWS, 128), F32),
            pltpu.VMEM((CH, CH), BF16),
            pltpu.VMEM((24 + ROWS, RP), F32),
            pltpu.VMEM((CH, RP), F32),
            pltpu.VMEM((CH, RP), BF16),
            pltpu.VMEM((CH, 2 * RP), F32),
            pltpu.VMEM((CH, RP), BF16),
            pltpu.VMEM((CH, 2048), BF16),
            pltpu.VMEM((CH, FP + FFL), F32),
            pltpu.VMEM((ROWS, FFL), BF16),
            pltpu.VMEM((SEQS, RP), F32),
            pltpu.SemaphoreType.DMA((14,)),
            pltpu.SemaphoreType.DMA((4, 2, 20)),
            pltpu.SemaphoreType.DMA((4, 2, 20)),
            pltpu.SemaphoreType.DMA((2, 8, CHUNKS)),
            pltpu.SemaphoreType.DMA((2, 8, CHUNKS)),
            pltpu.SemaphoreType.DMA((2, 5, CHUNKS)),
            pltpu.SemaphoreType.DMA((2, 5, CHUNKS)),
        ],
        compiler_params=pltpu.CompilerParams(
            collective_id=0, has_side_effects=True, vmem_limit_bytes=66_000_000
        ),
    )(*operands)


def shards(
    tokens,
    recurrence_norm_gain,
    output_gate_weight,
    recurrence_input_weight,
    convolution_taps,
    recurrence_gate_weight,
    input_gate_weight,
    base_decay_logit,
    token_log_decay,
    recurrence_output_weight,
    feedforward_norm_gain,
    feedforward_gate_weight,
    feedforward_up_weight,
    feedforward_down_weight,
):
    return layer(
        output_gate_weight.T,
        recurrence_input_weight.T,
        tokens,
        recurrence_output_weight,
        feedforward_gate_weight.T,
        feedforward_up_weight.T,
        feedforward_down_weight,
        recurrence_gate_weight.reshape(R, R),
        input_gate_weight.reshape(R, R),
        convolution_taps,
        base_decay_logit.reshape(1, R),
        token_log_decay.reshape(SEQS, LEN),
        recurrence_norm_gain.reshape(16, 128),
        feedforward_norm_gain.reshape(16, 128),
    )


def solution(mesh):
    in_specs = (
        P("fs", "tp"),
        P(),
        P("fs", "tp"),
        P("fs", "tp"),
        P(None, "tp"),
        P("tp", None, None),
        P("tp", None, None),
        P("tp"),
        P("fs"),
        P("tp", "fs"),
        P(),
        P("fs", "tp"),
        P("fs", "tp"),
        P("tp", "fs"),
    )
    return jax.shard_map(shards, mesh=mesh, in_specs=in_specs, out_specs=P("fs", "tp"), check_vma=False)
```

```python
import jax
import jax.numpy as jnp
from jax import lax
from jax.experimental import pallas as pl
from jax.experimental.pallas import tpu as pltpu
from jax.sharding import PartitionSpec as P

MESH = pl.DeviceIdType.MESH
F32 = jnp.float32
BF16 = jnp.bfloat16

LEN = 128
EPSILON = 1e-06
GATE_EXPONENT = 8.0

SIDE = 4
CHUNKS = 4
ROWS = 1024
CH = ROWS // CHUNKS
HALF = CH // 2
STEPS = LEN // CHUNKS
SEQS = 8
R = 352
RP = 384
FFL = 704
FP = 768
CB = 256
NT = (((1,), (1,)), ((), ()))

WGI_ROWS = (((0, 176), (176, 176)), ((RP, 176), (RP + 176, 176)))
WO_ROWS = (((0, 96), (96, 80)), ((176, 96), (272, 80)))
WFF_ROWS = (((0, 352), (352, 352)), ((FP, 352), (FP + 352, 352)))
WD_ROWS = (((0, 176), (176, 176)), ((352, 176), (528, 176)))


class Gather:
    def __init__(self, buf, rows, send, recv, pos, dev):
        self.buf, self.rows, self.send, self.recv, self.dev = buf, rows, send, recv, dev
        self.axes = (("x", "z"), ("z", "x"))
        self.pos = pos

    def block(self, part, i1, i2, half=None):
        z, x = (i2, i1) if part == 0 else (i1, i2)
        lo, hi = self.rows[part]
        span = pl.ds(lo[0], lo[1] + hi[1]) if half is None else pl.ds(*(lo, hi)[half])
        return self.buf.at[span, pl.ds(pl.multiple_of((z * SIDE + x) * 128, 128), 128)]

    def copy(self, view, part, k, to):
        return pltpu.make_async_remote_copy(
            src_ref=view,
            dst_ref=view,
            send_sem=self.send.at[part, k],
            recv_sem=self.recv.at[part, k],
            device_id=to,
            device_id_type=MESH,
        )

    def places(self, part):
        a1, a2 = self.axes[part]
        (m1, i1, p1), (m2, i2, p2) = self.pos[a1], self.pos[a2]
        far1, far2 = lax.rem(i1 + 2, SIDE), lax.rem(i2 + 2, SIDE)
        return (i1, m1, p1, far1), (i2, m2, p2, far2), self.dev[a1], self.dev[a2]

    def landing(self, part, k):
        first, second, _, _ = self.places(part)
        if k < 4:
            where = (first[1], first[2], first[3], first[3])[k]
            return self.block(part, where, second[0], None if k < 2 else k - 2)
        q, k = divmod(k - 4, 4)
        where = (second[1], second[2], second[3], second[3])[k]
        return self.block(part, first[q], where, None if k < 2 else k - 2)

    def arrived(self, part, k):
        self.copy(self.landing(part, k), part, k, self.dev["x"][0]).wait_recv()

    def onto_second(self, part, q):
        first, second, _, dev2 = self.places(part)
        view = self.block(part, first[q], second[0])
        self.copy(view, part, 4 + 4 * q, dev2[1]).start()
        self.copy(view, part, 5 + 4 * q, dev2[0]).start()

    def own(self):
        for part in (0, 1):
            first, second, dev1, _ = self.places(part)
            view = self.block(part, first[0], second[0])
            self.copy(view, part, 0, dev1[1]).start()
            self.copy(view, part, 1, dev1[0]).start()
        for part in (0, 1):
            self.onto_second(part, 0)

    def near(self):
        for part in (0, 1):
            first, second, dev1, _ = self.places(part)
            self.arrived(part, 0)
            self.copy(self.block(part, first[1], second[0], 0), part, 2, dev1[1]).start()
            self.arrived(part, 1)
            self.copy(self.block(part, first[2], second[0], 1), part, 3, dev1[0]).start()
        for part in (0, 1):
            self.onto_second(part, 1)
            self.onto_second(part, 2)

    def far(self):
        for part in (0, 1):
            self.arrived(part, 2)
            self.arrived(part, 3)
            self.onto_second(part, 3)

    def relay(self, q):
        for part in (0, 1):
            first, second, _, dev2 = self.places(part)
            self.arrived(part, 4 + 4 * q)
            self.copy(self.block(part, first[q], second[1], 0), part, 6 + 4 * q, dev2[1]).start()
            self.arrived(part, 5 + 4 * q)
            self.copy(self.block(part, first[q], second[2], 1), part, 7 + 4 * q, dev2[0]).start()

    def done(self):
        for part in (0, 1):
            for q in range(4):
                self.arrived(part, 6 + 4 * q)
                self.arrived(part, 7 + 4 * q)

    def drain(self):
        for part in (0, 1):
            for k in range(20):
                self.copy(self.landing(part, k), part, k, self.dev["x"][0]).wait_send()


class Spread:
    def __init__(self, buf, send, recv, y, core, dev):
        self.buf, self.send, self.recv, self.dev = buf, send, recv, dev
        (ym, yy, yp), far = y, lax.rem(y[1] + 2, SIDE)
        other = 1 - core
        self.own, self.minus, self.plus, self.far = (2 * v + core for v in (yy, ym, yp, far))
        self.others = [2 * v + other for v in (yy, ym, yp, far)]

    def view(self, block, c, half=None):
        if half is None:
            return self.buf.at[block, pl.ds(c * CH, CH), :]
        return self.buf.at[block, pl.ds(c * CH + half * HALF, HALF), :]

    def copy(self, view, k, c, to):
        return pltpu.make_async_remote_copy(
            src_ref=view,
            dst_ref=view,
            send_sem=self.send.at[k, c],
            recv_sem=self.recv.at[k, c],
            device_id=to,
            device_id_type=MESH,
        )

    def landing(self, k, c):
        return [
            (self.minus, None),
            (self.plus, None),
            (self.others[0], None),
            (self.far, 0),
            (self.far, 1),
            (self.others[1], None),
            (self.others[2], None),
            (self.others[3], None),
        ][k]

    def arrived(self, k, c):
        block, half = self.landing(k, c)
        self.copy(self.view(block, c, half), k, c, self.dev["core"]).wait_recv()

    def stage0(self, c):
        view = self.view(self.own, c)
        self.copy(view, 0, c, self.dev["y"][1]).start()
        self.copy(view, 1, c, self.dev["y"][0]).start()
        self.copy(view, 2, c, self.dev["core"]).start()

    def stage1(self, c):
        self.arrived(0, c)
        self.copy(self.view(self.minus, c, 0), 3, c, self.dev["y"][1]).start()
        self.copy(self.view(self.minus, c), 5, c, self.dev["core"]).start()
        self.arrived(1, c)
        self.copy(self.view(self.plus, c, 1), 4, c, self.dev["y"][0]).start()
        self.copy(self.view(self.plus, c), 6, c, self.dev["core"]).start()

    def stage2(self, c):
        self.arrived(3, c)
        self.arrived(4, c)
        self.copy(self.view(self.far, c), 7, c, self.dev["core"]).start()

    def stage3(self, c):
        for k in (2, 5, 6, 7):
            self.arrived(k, c)

    def drain(self, c):
        for k in range(8):
            block, half = self.landing(k, c)
            self.copy(self.view(block, c, half), k, c, self.dev["core"]).wait_send()


class Sum:
    def __init__(self, part, took, total, halves, finals, send, recv, y, core, dev):
        self.part, self.took, self.total = part, took, total
        self.halves, self.finals, self.send, self.recv, self.dev = halves, finals, send, recv, dev
        self.minus, self.own, self.plus = y
        self.far = lax.rem(y[1] + 2, SIDE)
        self.core = core

    def rows(self, c):
        return pl.ds(c * CH, CH)

    def half(self, c, h):
        return pl.ds(c * CH + h * HALF, HALF)

    def parts(self, k, c):
        if k == 0:
            return self.part.at[:, 1 - self.core, self.rows(c), :], self.took.at[:, self.rows(c), :], self.dev["core"]
        if k <= 2:
            return self.total.at[self.far, self.half(c, k - 1), :], self.halves.at[k - 1, c], self.dev["y"][2 - k]
        to = self.plus if k == 3 else self.minus
        return self.total.at[to, self.rows(c), :], self.finals.at[k - 3, self.rows(c), :], self.dev["y"][4 - k]

    def copy(self, k, c):
        src, dst, to = self.parts(k, c)
        return pltpu.make_async_remote_copy(
            src_ref=src,
            dst_ref=dst,
            send_sem=self.send.at[k, c],
            recv_sem=self.recv.at[k, c],
            device_id=to,
            device_id_type=MESH,
        )

    def stage0(self, c):
        self.copy(0, c).start()

    def stage1(self, c):
        self.copy(0, c).wait_recv()
        rows = self.rows(c)

        def add(target):
            self.total[target, rows, :] = (
                self.part[target, self.core, rows, :].astype(F32) + self.took[target, rows, :].astype(F32)
            ).astype(BF16)

        add(self.far)
        add(self.plus)
        self.copy(1, c).start()
        self.copy(2, c).start()
        add(self.minus)
        add(self.own)

    def stage2(self, c):
        for h, target in ((0, self.plus), (1, self.minus)):
            self.copy(1 + h, c).wait_recv()
            rows = self.half(c, h)
            self.total[target, rows, :] = (
                self.total[target, rows, :].astype(F32) + self.halves[h, c].astype(F32)
            ).astype(BF16)
        self.copy(3, c).start()
        self.copy(4, c).start()

    def stage3(self, c):
        self.copy(3, c).wait_recv()
        self.copy(4, c).wait_recv()
        rows = self.rows(c)
        return (
            self.total[self.own, rows, :].astype(F32)
            + self.finals[0, rows, :].astype(F32)
            + self.finals[1, rows, :].astype(F32)
        )

    def drain(self, c):
        for k in range(5):
            self.copy(k, c).wait_send()


def norm_chunk(full, gain, out, c):
    step = 16

    def body(i, carry):
        rows = pl.ds(pl.multiple_of(c * CH + i * step, step), step)
        here = pl.ds(pl.multiple_of(i * step, step), step)
        total = jnp.zeros((step, CB), F32)
        for b in range(8):
            v = full[b, rows, :].astype(F32)
            total = total + v * v
        scale = lax.rsqrt(jnp.sum(total, axis=1, keepdims=True) * (1.0 / 2048.0) + EPSILON)
        for b in range(8):
            v = full[b, rows, :].astype(F32) * scale
            for s in range(2):
                g = gain[2 * b + s : 2 * b + s + 1, :]
                lo = b * CB + s * 128
                out[here, lo : lo + 128] = (v[:, s * 128 : s * 128 + 128] * g).astype(BF16)
        return carry

    lax.fori_loop(0, CH // step, body, 0, unroll=2)


def order(shape, major):
    to = lax.broadcasted_iota(jnp.int32, shape, 0)
    source = lax.broadcasted_iota(jnp.int32, shape, 1)
    if major == "time":
        wanted = lax.rem(to, SEQS) * STEPS + to // SEQS
    else:
        wanted = lax.rem(to, STEPS) * SEQS + to // STEPS
    return jnp.where(source == wanted, 1.0, 0.0).astype(BF16)


def kernel(
    wg_hbm, wi_hbm, tok_hbm, wo_hbm, wfg_hbm, wfu_hbm, wd_hbm,
    gr_hbm, gi_hbm, taps_hbm, base_hbm, ld_hbm, gain1_hbm, gain2_hbm,
    out,
    full1, full2, wgi, wo, wff, wd,
    part1, took1, total1, halves1, finals1,
    part2, took2, total2, halves2, finals2,
    tokv, grv, giv, tapsv, basev, ldv, gain1, gain2,
    gm, small, ldb, perm,
    feat, proj, mixed, gl, carried, nrm, ffo, hid, state,
    local_sem, w_send, w_recv, a_send, a_recv, s_send, s_recv,
):
    fs, tp = lax.axis_index("fs"), lax.axis_index("tp")
    iz, ix = fs // SIDE, lax.rem(fs, SIDE)
    iy, core = tp // 2, lax.rem(tp, 2)

    def ring(i):
        return lax.rem(i + SIDE - 1, SIDE), i, lax.rem(i + 1, SIDE)

    pos = {"x": ring(ix), "z": ring(iz)}
    y = ring(iy)
    dev = {
        "x": tuple({"fs": iz * SIDE + pos["x"][k]} for k in (0, 2)),
        "z": tuple({"fs": pos["z"][k] * SIDE + ix} for k in (0, 2)),
        "y": tuple({"tp": 2 * y[k] + core} for k in (0, 2)),
        "core": {"tp": 2 * iy + 1 - core},
    }

    barrier = pltpu.get_barrier_semaphore()
    for to in (*dev["x"], *dev["z"], *dev["y"], dev["core"]):
        pl.semaphore_signal(barrier, inc=1, device_id=to, device_id_type=MESH)

    cols = pl.ds(pl.multiple_of(fs * 128, 128), 128)
    local = [
        pltpu.make_async_copy(src, dst, local_sem.at[n])
        for n, (src, dst) in enumerate(
            (
                (wg_hbm, wgi.at[pl.ds(0, R), cols]),
                (wi_hbm, wgi.at[pl.ds(RP, R), cols]),
                (tok_hbm, tokv),
                (wo_hbm, wo.at[pl.ds(0, R), cols]),
                (wfg_hbm, wff.at[pl.ds(0, FFL), cols]),
                (wfu_hbm, wff.at[pl.ds(FP, FFL), cols]),
                (wd_hbm, wd.at[:, cols]),
                (gr_hbm, grv),
                (gi_hbm, giv),
                (taps_hbm, tapsv),
                (base_hbm, basev),
                (ld_hbm, ldv),
                (gain1_hbm, gain1),
                (gain2_hbm, gain2),
            )
        )
    ]
    for copy in local:
        copy.start()
    wgi[R:RP, :] = jnp.zeros((RP - R, 2048), BF16)
    wgi[RP + R :, :] = jnp.zeros((RP - R, 2048), BF16)
    wo[R:RP, :] = jnp.zeros((RP - R, 2048), BF16)
    wff[FFL:FP, :] = jnp.zeros((FP - FFL, 2048), BF16)
    perm[...] = order((CH, CH), "time")

    gathers = [
        Gather(buf, rows, w_send.at[m], w_recv.at[m], pos, dev)
        for m, (buf, rows) in enumerate(((wgi, WGI_ROWS), (wo, WO_ROWS), (wff, WFF_ROWS), (wd, WD_ROWS)))
    ]
    g_wgi, g_wo, g_wff, g_wd = gathers
    spread1 = Spread(full1, a_send.at[0], a_recv.at[0], y, core, dev)
    spread2 = Spread(full2, a_send.at[1], a_recv.at[1], y, core, dev)
    sum1 = Sum(part1, took1, total1, halves1, finals1, s_send.at[0], s_recv.at[0], y, core, dev)
    sum2 = Sum(part2, took2, total2, halves2, finals2, s_send.at[1], s_recv.at[1], y, core, dev)

    def reordered(c):
        pieces = [tokv[s * LEN + c * STEPS : s * LEN + (c + 1) * STEPS, :] for s in range(SEQS)]
        full1[tp, c * CH : (c + 1) * CH, :] = jnp.dot(
            perm[...], jnp.concatenate(pieces, axis=0), preferred_element_type=F32
        ).astype(BF16)

    local[2].wait()
    for c in range(CHUNKS):
        reordered(c)
    local[0].wait()
    local[1].wait()
    pl.semaphore_wait(barrier, 7)

    def small_operands():
        for n in range(7, 14):
            local[n].wait()
        gm[...] = jnp.zeros_like(gm)
        gm[0:R, 0:R] = grv[...]
        gm[0:R, RP : RP + R] = giv[...]
        small[...] = jnp.zeros_like(small)
        small[0:4, 0:R] = tapsv[...]
        small[4:5, 0:R] = -GATE_EXPONENT * jax.nn.softplus(-basev[...].reshape(1, R))
        for t in range(LEN):
            ldb[8 * t : 8 * t + 8, :] = jnp.broadcast_to(ldv[:, t : t + 1], (SEQS, 128))
        feat[0:24, :] = jnp.zeros((24, RP), F32)
        state[...] = jnp.zeros_like(state)

    def norm1(c):
        spread1.stage3(c)
        norm_chunk(full1, gain1, nrm, c)

    def project(c):
        base = c * CH
        projected = lax.dot_general(nrm[...], wgi[...], NT, preferred_element_type=F32)
        proj[...] = projected[:, :RP]
        feat[pl.ds(base + 24, CH), :] = projected[:, RP:].astype(BF16).astype(F32)

    def scan(c):
        base = c * CH

        def taps(i, carry):
            r = pl.multiple_of(i * 32, 32)
            summed = small[0:1, :] * feat[pl.ds(base + r, 32), :]
            for k in range(1, 4):
                summed = summed + small[k : k + 1, :] * feat[pl.ds(base + r + 8 * k, 32), :]
            mixed[pl.ds(r, 32), :] = summed.astype(BF16)
            return carry

        lax.fori_loop(0, CH // 32, taps, 0, unroll=2)
        gl[...] = jnp.dot(mixed[...], gm[...], preferred_element_type=F32)

        def steps(i, h):
            r = pl.multiple_of(i * 32, 32)
            rows = pl.ds(r, 32)
            recur = jax.nn.sigmoid(gl[rows, :RP])
            inject = jax.nn.sigmoid(gl[rows, RP:])
            struck = ldb[pl.ds(base + r, 32), :]
            log_decay = small[4:5, :] * recur + jnp.concatenate([struck] * 3, axis=1)
            decay = jnp.exp(log_decay)
            twice = 2.0 * log_decay
            near = -twice * (1.0 + twice * (0.5 + twice * (1.0 / 6.0 + twice * (1.0 / 24.0 + twice * (1.0 / 120.0)))))
            rest = jnp.where(twice > -0.1, near, 1.0 - decay * decay)
            driven = jnp.sqrt(rest) * (inject * mixed[rows, :].astype(F32))
            states = []
            for s in range(4):
                h = decay[8 * s : 8 * s + 8] * h + driven[8 * s : 8 * s + 8]
                states.append(h)
            carried[rows, :] = (jnp.concatenate(states, axis=0) * jax.nn.gelu(proj[rows, :])).astype(BF16)
            return h

        state[...] = lax.fori_loop(0, CH // 32, steps, state[...])

    def mix_out(c):
        rows = pl.ds(c * CH, CH)
        for j in range(8):
            part1[j // 2, j % 2, rows, :] = jnp.dot(
                carried[...], wo[:, j * CB : (j + 1) * CB], preferred_element_type=F32
            ).astype(BF16)
        sum1.stage0(c)

    def settle(c):
        rows = pl.ds(c * CH, CH)
        full2[tp, rows, :] = (full1[tp, rows, :].astype(F32) + sum1.stage3(c)).astype(BF16)
        spread2.stage0(c)

    def norm2(c):
        spread2.stage3(c)
        norm_chunk(full2, gain2, nrm, c)

    def up(c):
        ffo[...] = lax.dot_general(nrm[...], wff[...], NT, preferred_element_type=F32)

    def act(c):
        base = c * CH

        def body(i, carry):
            r = pl.multiple_of(i * 16, 16)
            rows = pl.ds(r, 16)
            hid[pl.ds(base + r, 16), :] = (jax.nn.silu(ffo[rows, :FFL]) * ffo[rows, FP:]).astype(BF16)
            return carry

        lax.fori_loop(0, CH // 16, body, 0, unroll=2)

    def down(c):
        rows = pl.ds(c * CH, CH)
        for j in range(8):
            part2[j // 2, j % 2, rows, :] = jnp.dot(
                hid[rows, :], wd[:, j * CB : (j + 1) * CB], preferred_element_type=F32
            ).astype(BF16)
        sum2.stage0(c)

    def finish(c):
        rows = pl.ds(c * CH, CH)
        layer_out = (full2[tp, rows, :].astype(F32) + sum2.stage3(c)).astype(BF16)
        ordered = jnp.dot(perm[...], layer_out, preferred_element_type=F32).astype(BF16)
        for s in range(SEQS):
            out[pl.ds(s * LEN + c * STEPS, STEPS), :] = ordered[s * STEPS : (s + 1) * STEPS]

    g_wgi.own()
    spread1.stage0(0)
    local[3].wait()
    g_wo.own()
    spread1.stage0(1)
    spread1.stage0(3)
    spread1.stage0(2)
    small_operands()
    g_wgi.near()
    g_wo.near()
    spread1.stage1(3)
    g_wgi.far()
    spread1.stage1(1)
    g_wgi.relay(2)
    g_wo.far()
    spread1.stage1(2)
    g_wgi.relay(0)
    spread1.stage1(0)
    g_wgi.relay(1)
    spread1.stage2(3)
    g_wgi.relay(3)
    g_wo.relay(3)
    spread1.stage2(2)
    g_wo.relay(2)
    g_wo.relay(0)
    g_wo.relay(1)
    spread1.stage2(1)
    local[4].wait()
    local[5].wait()
    g_wff.own()
    spread1.stage2(0)
    norm1(0)
    g_wgi.done()
    project(0)
    scan(0)
    g_wo.done()
    mix_out(0)
    norm1(1)
    project(1)
    sum1.stage1(0)
    g_wff.near()
    scan(1)
    mix_out(1)
    sum1.stage1(1)
    sum1.stage2(0)
    g_wff.relay(0)
    g_wff.far()
    local[6].wait()
    g_wd.own()
    norm1(2)
    project(2)
    sum1.stage2(1)
    scan(2)
    mix_out(2)
    settle(0)
    norm1(3)
    project(3)
    sum1.stage1(2)
    settle(1)
    g_wff.relay(2)
    scan(3)
    mix_out(3)
    g_wff.relay(1)
    sum1.stage2(2)
    sum1.stage1(3)
    g_wff.relay(3)
    for c in range(CHUNKS):
        spread1.drain(c)
    g_wd.near()
    spread2.stage1(0)
    spread2.stage1(1)
    g_wgi.drain()
    g_wo.drain()
    settle(2)
    sum1.stage2(3)
    spread2.stage2(0)
    norm2(0)
    spread2.stage2(1)
    g_wff.done()
    up(0)
    spread2.stage1(2)
    g_wd.far()
    act(0)
    norm2(1)
    g_wd.relay(1)
    up(1)
    g_wd.relay(2)
    settle(3)
    spread2.stage2(2)
    act(1)
    g_wd.relay(0)
    g_wd.relay(3)
    norm2(2)
    up(2)
    act(2)
    spread2.stage1(3)
    g_wd.done()
    down(0)
    down(1)
    down(2)
    sum2.stage1(0)
    sum2.stage1(1)
    sum2.stage1(2)
    spread2.stage2(3)
    g_wff.drain()
    sum2.stage2(0)
    norm2(3)
    up(3)
    sum2.stage2(2)
    act(3)
    down(3)
    perm[...] = order((CH, CH), "sequence")
    g_wd.drain()
    finish(0)
    sum2.stage1(3)
    sum2.stage2(1)
    for c in range(CHUNKS):
        sum1.drain(c)
    finish(2)
    for c in range(CHUNKS):
        spread2.drain(c)
    sum2.stage2(3)
    finish(1)
    finish(3)

    for c in range(CHUNKS):
        sum2.drain(c)


def layer(*operands):
    sums = [
        pltpu.VMEM((SIDE, 2, ROWS, CB), BF16),
        pltpu.VMEM((SIDE, ROWS, CB), BF16),
        pltpu.VMEM((SIDE, ROWS, CB), BF16),
        pltpu.VMEM((2, CHUNKS, HALF, CB), BF16),
        pltpu.VMEM((2, ROWS, CB), BF16),
    ]
    return pl.pallas_call(
        kernel,
        out_shape=jax.ShapeDtypeStruct((ROWS, CB), BF16),
        in_specs=[pl.BlockSpec(memory_space=pl.ANY)] * len(operands),
        out_specs=pl.BlockSpec(memory_space=pltpu.VMEM),
        scratch_shapes=[
            pltpu.VMEM((8, ROWS, CB), BF16),
            pltpu.VMEM((8, ROWS, CB), BF16),
            pltpu.VMEM((2 * RP, 2048), BF16),
            pltpu.VMEM((RP, 2048), BF16),
            pltpu.VMEM((FP + FFL, 2048), BF16),
            pltpu.VMEM((FFL, 2048), BF16),
            *sums,
            *sums,
            pltpu.VMEM((ROWS, CB), BF16),
            pltpu.VMEM((R, R), BF16),
            pltpu.VMEM((R, R), BF16),
            pltpu.VMEM((4, R), F32),
            pltpu.VMEM((R,), F32),
            pltpu.VMEM((SEQS, LEN), F32),
            pltpu.VMEM((16, 128), F32),
            pltpu.VMEM((16, 128), F32),
            pltpu.VMEM((RP, 2 * RP), BF16),
            pltpu.VMEM((8, RP), F32),
            pltpu.VMEM((ROWS, 128), F32),
            pltpu.VMEM((CH, CH), BF16),
            pltpu.VMEM((24 + ROWS, RP), F32),
            pltpu.VMEM((CH, RP), F32),
            pltpu.VMEM((CH, RP), BF16),
            pltpu.VMEM((CH, 2 * RP), F32),
            pltpu.VMEM((CH, RP), BF16),
            pltpu.VMEM((CH, 2048), BF16),
            pltpu.VMEM((CH, FP + FFL), F32),
            pltpu.VMEM((ROWS, FFL), BF16),
            pltpu.VMEM((SEQS, RP), F32),
            pltpu.SemaphoreType.DMA((14,)),
            pltpu.SemaphoreType.DMA((4, 2, 20)),
            pltpu.SemaphoreType.DMA((4, 2, 20)),
            pltpu.SemaphoreType.DMA((2, 8, CHUNKS)),
            pltpu.SemaphoreType.DMA((2, 8, CHUNKS)),
            pltpu.SemaphoreType.DMA((2, 5, CHUNKS)),
            pltpu.SemaphoreType.DMA((2, 5, CHUNKS)),
        ],
        compiler_params=pltpu.CompilerParams(
            collective_id=0, has_side_effects=True, vmem_limit_bytes=66_000_000
        ),
    )(*operands)


def shards(
    tokens,
    recurrence_norm_gain,
    output_gate_weight,
    recurrence_input_weight,
    convolution_taps,
    recurrence_gate_weight,
    input_gate_weight,
    base_decay_logit,
    token_log_decay,
    recurrence_output_weight,
    feedforward_norm_gain,
    feedforward_gate_weight,
    feedforward_up_weight,
    feedforward_down_weight,
):
    return layer(
        output_gate_weight.T,
        recurrence_input_weight.T,
        tokens,
        recurrence_output_weight,
        feedforward_gate_weight.T,
        feedforward_up_weight.T,
        feedforward_down_weight,
        recurrence_gate_weight.reshape(R, R),
        input_gate_weight.reshape(R, R),
        convolution_taps,
        base_decay_logit,
        token_log_decay.reshape(SEQS, LEN),
        recurrence_norm_gain.reshape(16, 128),
        feedforward_norm_gain.reshape(16, 128),
    )


def solution(mesh):
    in_specs = (
        P("fs", "tp"),
        P(),
        P("fs", "tp"),
        P("fs", "tp"),
        P(None, "tp"),
        P("tp", None, None),
        P("tp", None, None),
        P("tp"),
        P("fs"),
        P("tp", "fs"),
        P(),
        P("fs", "tp"),
        P("fs", "tp"),
        P("tp", "fs"),
    )
    return jax.shard_map(shards, mesh=mesh, in_specs=in_specs, out_specs=P("fs", "tp"), check_vma=False)
```

```python
import jax
import jax.numpy as jnp
from jax import lax
from jax.experimental import pallas as pl
from jax.experimental.pallas import tpu as pltpu
from jax.sharding import PartitionSpec as P

MESH = pl.DeviceIdType.MESH
F32 = jnp.float32
BF16 = jnp.bfloat16

LEN = 128
EPSILON = 1e-06
GATE_EXPONENT = 8.0

SIDE = 4
CHUNKS = 4
ROWS = 1024
CH = ROWS // CHUNKS
HALF = CH // 2
STEPS = LEN // CHUNKS
SEQS = 8
R = 352
RP = 384
FFL = 704
FP = 768
CB = 256
NT = (((1,), (1,)), ((), ()))

WGI_ROWS = (((0, 176), (176, 176)), ((RP, 176), (RP + 176, 176)))
WO_ROWS = (((0, 96), (96, 80)), ((176, 96), (272, 80)))
WFF_ROWS = (((0, 352), (352, 352)), ((FP, 352), (FP + 352, 352)))
WD_ROWS = (((0, 176), (176, 176)), ((352, 176), (528, 176)))


class Gather:
    def __init__(self, buf, rows, send, recv, pos, dev):
        self.buf, self.rows, self.send, self.recv, self.dev = buf, rows, send, recv, dev
        self.axes = (("x", "z"), ("z", "x"))
        self.pos = pos

    def block(self, part, i1, i2, half=None):
        z, x = (i2, i1) if part == 0 else (i1, i2)
        lo, hi = self.rows[part]
        span = pl.ds(lo[0], lo[1] + hi[1]) if half is None else pl.ds(*(lo, hi)[half])
        return self.buf.at[span, pl.ds(pl.multiple_of((z * SIDE + x) * 128, 128), 128)]

    def group(self, k):
        if k < 4:
            return k // 2
        return 6 if (k - 4) % 4 >= 2 else 2 + (k - 4) // 4

    def copy(self, view, part, k, to):
        return pltpu.make_async_remote_copy(
            src_ref=view,
            dst_ref=view,
            send_sem=self.send,
            recv_sem=self.recv.at[self.group(k)],
            device_id=to,
            device_id_type=MESH,
        )

    def blocks(self, count, group):
        (lo, hi), _ = self.rows
        view = self.buf.at[pl.ds(0, 2 * (lo[1] + hi[1])), pl.ds(0, 128 * count)]
        return pltpu.make_async_remote_copy(
            src_ref=view,
            dst_ref=view,
            send_sem=self.send,
            recv_sem=self.recv.at[group],
            device_id=self.dev["x"][0],
            device_id_type=MESH,
        )

    def places(self, part):
        a1, a2 = self.axes[part]
        (m1, i1, p1), (m2, i2, p2) = self.pos[a1], self.pos[a2]
        far1, far2 = lax.rem(i1 + 2, SIDE), lax.rem(i2 + 2, SIDE)
        return (i1, m1, p1, far1), (i2, m2, p2, far2), self.dev[a1], self.dev[a2]

    def onto_second(self, part, q):
        first, second, _, dev2 = self.places(part)
        view = self.block(part, first[q], second[0])
        self.copy(view, part, 4 + 4 * q, dev2[1]).start()
        self.copy(view, part, 5 + 4 * q, dev2[0]).start()

    def own(self):
        for part in (0, 1):
            first, second, dev1, _ = self.places(part)
            view = self.block(part, first[0], second[0])
            self.copy(view, part, 0, dev1[1]).start()
            self.copy(view, part, 1, dev1[0]).start()
        for part in (0, 1):
            self.onto_second(part, 0)

    def near(self):
        self.blocks(2, 0).wait_recv()
        for part in (0, 1):
            first, second, dev1, _ = self.places(part)
            self.copy(self.block(part, first[1], second[0], 0), part, 2, dev1[1]).start()
            self.copy(self.block(part, first[2], second[0], 1), part, 3, dev1[0]).start()
        for part in (0, 1):
            self.onto_second(part, 1)
            self.onto_second(part, 2)

    def far(self):
        self.blocks(1, 1).wait_recv()
        for part in (0, 1):
            self.onto_second(part, 3)

    def relay(self, q):
        self.blocks(2, 2 + q).wait_recv()
        for part in (0, 1):
            first, second, _, dev2 = self.places(part)
            self.copy(self.block(part, first[q], second[1], 0), part, 6 + 4 * q, dev2[1]).start()
            self.copy(self.block(part, first[q], second[2], 1), part, 7 + 4 * q, dev2[0]).start()

    def done(self):
        self.blocks(4, 6).wait_recv()

    def drain(self):
        self.blocks(15, 0).wait_send()


class Spread:
    def __init__(self, buf, send, recv, y, core, dev):
        self.buf, self.send, self.recv, self.dev = buf, send, recv, dev
        (ym, yy, yp), far = y, lax.rem(y[1] + 2, SIDE)
        other = 1 - core
        self.own, self.minus, self.plus, self.far = (2 * v + core for v in (yy, ym, yp, far))
        self.others = [2 * v + other for v in (yy, ym, yp, far)]

    def view(self, block, c, half=None):
        if half is None:
            return self.buf.at[block, pl.ds(c * CH, CH), :]
        return self.buf.at[block, pl.ds(c * CH + half * HALF, HALF), :]

    def copy(self, view, k, c, to):
        return pltpu.make_async_remote_copy(
            src_ref=view,
            dst_ref=view,
            send_sem=self.send,
            recv_sem=self.recv.at[(0, 0, 2, 1, 1, 2, 2, 2)[k], c],
            device_id=to,
            device_id_type=MESH,
        )

    def arrived(self, count, group, c):
        view = self.buf.at[pl.ds(0, count), pl.ds(c * CH, CH), :]
        pltpu.make_async_remote_copy(
            src_ref=view,
            dst_ref=view,
            send_sem=self.send,
            recv_sem=self.recv.at[group, c],
            device_id=self.dev["core"],
            device_id_type=MESH,
        ).wait_recv()

    def stage0(self, c):
        view = self.view(self.own, c)
        self.copy(view, 0, c, self.dev["y"][1]).start()
        self.copy(view, 1, c, self.dev["y"][0]).start()
        self.copy(view, 2, c, self.dev["core"]).start()

    def stage1(self, c):
        self.arrived(2, 0, c)
        self.copy(self.view(self.minus, c, 0), 3, c, self.dev["y"][1]).start()
        self.copy(self.view(self.minus, c), 5, c, self.dev["core"]).start()
        self.copy(self.view(self.plus, c, 1), 4, c, self.dev["y"][0]).start()
        self.copy(self.view(self.plus, c), 6, c, self.dev["core"]).start()

    def stage2(self, c):
        self.arrived(1, 1, c)
        self.copy(self.view(self.far, c), 7, c, self.dev["core"]).start()

    def stage3(self, c):
        self.arrived(4, 2, c)

    def drain(self):
        view = self.buf.at[pl.ds(0, 7)]
        pltpu.make_async_remote_copy(
            src_ref=view,
            dst_ref=view,
            send_sem=self.send,
            recv_sem=self.recv.at[0, 0],
            device_id=self.dev["core"],
            device_id_type=MESH,
        ).wait_send()


class Sum:
    def __init__(self, part, took, total, halves, finals, send, recv, y, core, dev):
        self.part, self.took, self.total = part, took, total
        self.halves, self.finals, self.send, self.recv, self.dev = halves, finals, send, recv, dev
        self.minus, self.own, self.plus = y
        self.far = lax.rem(y[1] + 2, SIDE)
        self.core = core

    def rows(self, c):
        return pl.ds(c * CH, CH)

    def half(self, c, h):
        return pl.ds(c * CH + h * HALF, HALF)

    def parts(self, k, c):
        if k == 0:
            return self.part.at[:, 1 - self.core, self.rows(c), :], self.took.at[:, self.rows(c), :], self.dev["core"]
        if k <= 2:
            return self.total.at[self.far, self.half(c, k - 1), :], self.halves.at[k - 1, c], self.dev["y"][2 - k]
        to = self.plus if k == 3 else self.minus
        return self.total.at[to, self.rows(c), :], self.finals.at[k - 3, self.rows(c), :], self.dev["y"][4 - k]

    def copy(self, k, c):
        src, dst, to = self.parts(k, c)
        return pltpu.make_async_remote_copy(
            src_ref=src,
            dst_ref=dst,
            send_sem=self.send,
            recv_sem=self.recv.at[(k + 1) // 2, c],
            device_id=to,
            device_id_type=MESH,
        )

    def arrived(self, view, group, c):
        pltpu.make_async_remote_copy(
            src_ref=view,
            dst_ref=view,
            send_sem=self.send,
            recv_sem=self.recv.at[group, c],
            device_id=self.dev["core"],
            device_id_type=MESH,
        ).wait_recv()

    def stage0(self, c):
        self.copy(0, c).start()

    def stage1(self, c):
        self.copy(0, c).wait_recv()
        rows = self.rows(c)

        def add(target):
            self.total[target, rows, :] = (
                self.part[target, self.core, rows, :].astype(F32) + self.took[target, rows, :].astype(F32)
            ).astype(BF16)

        add(self.far)
        add(self.plus)
        self.copy(1, c).start()
        self.copy(2, c).start()
        add(self.minus)
        add(self.own)

    def stage2(self, c):
        self.arrived(self.halves.at[:, c], 1, c)
        for h, target in ((0, self.plus), (1, self.minus)):
            rows = self.half(c, h)
            self.total[target, rows, :] = (
                self.total[target, rows, :].astype(F32) + self.halves[h, c].astype(F32)
            ).astype(BF16)
        self.copy(3, c).start()
        self.copy(4, c).start()

    def stage3(self, c):
        rows = self.rows(c)
        self.arrived(self.finals.at[:, rows, :], 2, c)
        return (
            self.total[self.own, rows, :].astype(F32)
            + self.finals[0, rows, :].astype(F32)
            + self.finals[1, rows, :].astype(F32)
        )

    def drain(self, like):
        view = like.at[pl.ds(0, 7)]
        pltpu.make_async_remote_copy(
            src_ref=view,
            dst_ref=view,
            send_sem=self.send,
            recv_sem=self.recv.at[0, 0],
            device_id=self.dev["core"],
            device_id_type=MESH,
        ).wait_send()


def norm_chunk(full, gain, out, c):
    step = 16

    def body(i, carry):
        rows = pl.ds(pl.multiple_of(c * CH + i * step, step), step)
        here = pl.ds(pl.multiple_of(i * step, step), step)
        total = jnp.zeros((step, CB), F32)
        for b in range(8):
            v = full[b, rows, :].astype(F32)
            total = total + v * v
        scale = lax.rsqrt(jnp.sum(total, axis=1, keepdims=True) * (1.0 / 2048.0) + EPSILON)
        for b in range(8):
            v = full[b, rows, :].astype(F32) * scale
            for s in range(2):
                g = gain[2 * b + s : 2 * b + s + 1, :]
                lo = b * CB + s * 128
                out[here, lo : lo + 128] = (v[:, s * 128 : s * 128 + 128] * g).astype(BF16)
        return carry

    lax.fori_loop(0, CH // step, body, 0, unroll=2)


def order(shape, major):
    to = lax.broadcasted_iota(jnp.int32, shape, 0)
    source = lax.broadcasted_iota(jnp.int32, shape, 1)
    if major == "time":
        wanted = lax.rem(to, SEQS) * STEPS + to // SEQS
    else:
        wanted = lax.rem(to, STEPS) * SEQS + to // STEPS
    return jnp.where(source == wanted, 1.0, 0.0).astype(BF16)


def kernel(
    wg_hbm, wi_hbm, tok_hbm, wo_hbm, wfg_hbm, wfu_hbm, wd_hbm,
    gr_hbm, gi_hbm, taps_hbm, base_hbm, ld_hbm, gain1_hbm, gain2_hbm,
    out,
    full1, full2, wgi, wo, wff, wd,
    part1, took1, total1, halves1, finals1,
    part2, took2, total2, halves2, finals2,
    tokv, grv, giv, tapsv, basev, ldv, gain1, gain2,
    gm, small, ldb, perm,
    feat, proj, mixed, gl, carried, nrm, ffo, hid, state,
    local_sem, w_send, w_recv, a_send, a_recv, s_send, s_recv,
):
    fs, tp = lax.axis_index("fs"), lax.axis_index("tp")
    iz, ix = fs // SIDE, lax.rem(fs, SIDE)
    iy, core = tp // 2, lax.rem(tp, 2)

    def ring(i):
        return lax.rem(i + SIDE - 1, SIDE), i, lax.rem(i + 1, SIDE)

    pos = {"x": ring(ix), "z": ring(iz)}
    y = ring(iy)
    dev = {
        "x": tuple({"fs": iz * SIDE + pos["x"][k]} for k in (0, 2)),
        "z": tuple({"fs": pos["z"][k] * SIDE + ix} for k in (0, 2)),
        "y": tuple({"tp": 2 * y[k] + core} for k in (0, 2)),
        "core": {"tp": 2 * iy + 1 - core},
    }

    barrier = pltpu.get_barrier_semaphore()
    for to in (*dev["x"], *dev["z"], *dev["y"], dev["core"]):
        pl.semaphore_signal(barrier, inc=1, device_id=to, device_id_type=MESH)

    cols = pl.ds(pl.multiple_of(fs * 128, 128), 128)
    local = [
        pltpu.make_async_copy(src, dst, local_sem.at[n])
        for n, (src, dst) in enumerate(
            (
                (wg_hbm, wgi.at[pl.ds(0, R), cols]),
                (wi_hbm, wgi.at[pl.ds(RP, R), cols]),
                (tok_hbm, tokv),
                (wo_hbm, wo.at[pl.ds(0, R), cols]),
                (wfg_hbm, wff.at[pl.ds(0, FFL), cols]),
                (wfu_hbm, wff.at[pl.ds(FP, FFL), cols]),
                (wd_hbm, wd.at[:, cols]),
                (gr_hbm, grv),
                (gi_hbm, giv),
                (taps_hbm, tapsv),
                (base_hbm, basev),
                (ld_hbm, ldv),
                (gain1_hbm, gain1),
                (gain2_hbm, gain2),
            )
        )
    ]
    for copy in local:
        copy.start()
    wgi[R:RP, :] = jnp.zeros((RP - R, 2048), BF16)
    wgi[RP + R :, :] = jnp.zeros((RP - R, 2048), BF16)
    wo[R:RP, :] = jnp.zeros((RP - R, 2048), BF16)
    wff[FFL:FP, :] = jnp.zeros((FP - FFL, 2048), BF16)
    perm[...] = order((CH, CH), "time")

    gathers = [
        Gather(buf, rows, w_send.at[m], w_recv.at[m], pos, dev)
        for m, (buf, rows) in enumerate(((wgi, WGI_ROWS), (wo, WO_ROWS), (wff, WFF_ROWS), (wd, WD_ROWS)))
    ]
    g_wgi, g_wo, g_wff, g_wd = gathers
    spread1 = Spread(full1, a_send.at[0], a_recv.at[0], y, core, dev)
    spread2 = Spread(full2, a_send.at[1], a_recv.at[1], y, core, dev)
    sum1 = Sum(part1, took1, total1, halves1, finals1, s_send.at[0], s_recv.at[0], y, core, dev)
    sum2 = Sum(part2, took2, total2, halves2, finals2, s_send.at[1], s_recv.at[1], y, core, dev)

    def reordered(c):
        pieces = [tokv[s * LEN + c * STEPS : s * LEN + (c + 1) * STEPS, :] for s in range(SEQS)]
        full1[tp, c * CH : (c + 1) * CH, :] = jnp.dot(
            perm[...], jnp.concatenate(pieces, axis=0), preferred_element_type=F32
        ).astype(BF16)

    local[2].wait()
    for c in range(CHUNKS):
        reordered(c)
    local[0].wait()
    local[1].wait()
    pl.semaphore_wait(barrier, 7)

    def small_operands():
        for n in range(7, 14):
            local[n].wait()
        gm[...] = jnp.zeros_like(gm)
        gm[0:R, 0:R] = grv[...]
        gm[0:R, RP : RP + R] = giv[...]
        small[...] = jnp.zeros_like(small)
        small[0:4, 0:R] = tapsv[...]
        small[4:5, 0:R] = -GATE_EXPONENT * jax.nn.softplus(-basev[...].reshape(1, R))
        for t in range(LEN):
            ldb[8 * t : 8 * t + 8, :] = jnp.broadcast_to(ldv[:, t : t + 1], (SEQS, 128))
        feat[0:24, :] = jnp.zeros((24, RP), F32)
        state[...] = jnp.zeros_like(state)

    def norm1(c):
        spread1.stage3(c)
        norm_chunk(full1, gain1, nrm, c)

    def project(c):
        base = c * CH
        projected = lax.dot_general(nrm[...], wgi[...], NT, preferred_element_type=F32)
        proj[...] = projected[:, :RP]
        feat[pl.ds(base + 24, CH), :] = projected[:, RP:].astype(BF16).astype(F32)

    def scan(c):
        base = c * CH

        def taps(i, carry):
            r = pl.multiple_of(i * 32, 32)
            summed = small[0:1, :] * feat[pl.ds(base + r, 32), :]
            for k in range(1, 4):
                summed = summed + small[k : k + 1, :] * feat[pl.ds(base + r + 8 * k, 32), :]
            mixed[pl.ds(r, 32), :] = summed.astype(BF16)
            return carry

        lax.fori_loop(0, CH // 32, taps, 0, unroll=2)
        gl[...] = jnp.dot(mixed[...], gm[...], preferred_element_type=F32)

        def steps(i, h):
            r = pl.multiple_of(i * 32, 32)
            rows = pl.ds(r, 32)
            recur = jax.nn.sigmoid(gl[rows, :RP])
            inject = jax.nn.sigmoid(gl[rows, RP:])
            struck = ldb[pl.ds(base + r, 32), :]
            log_decay = small[4:5, :] * recur + jnp.concatenate([struck] * 3, axis=1)
            decay = jnp.exp(log_decay)
            twice = 2.0 * log_decay
            near = -twice * (1.0 + twice * (0.5 + twice * (1.0 / 6.0 + twice * (1.0 / 24.0 + twice * (1.0 / 120.0)))))
            rest = jnp.where(twice > -0.1, near, 1.0 - decay * decay)
            driven = jnp.sqrt(rest) * (inject * mixed[rows, :].astype(F32))
            states = []
            for s in range(4):
                h = decay[8 * s : 8 * s + 8] * h + driven[8 * s : 8 * s + 8]
                states.append(h)
            carried[rows, :] = (jnp.concatenate(states, axis=0) * jax.nn.gelu(proj[rows, :])).astype(BF16)
            return h

        state[...] = lax.fori_loop(0, CH // 32, steps, state[...])

    def mix_out(c):
        rows = pl.ds(c * CH, CH)
        for j in range(8):
            part1[j // 2, j % 2, rows, :] = jnp.dot(
                carried[...], wo[:, j * CB : (j + 1) * CB], preferred_element_type=F32
            ).astype(BF16)
        sum1.stage0(c)

    def settle(c):
        rows = pl.ds(c * CH, CH)
        full2[tp, rows, :] = (full1[tp, rows, :].astype(F32) + sum1.stage3(c)).astype(BF16)
        spread2.stage0(c)

    def norm2(c):
        spread2.stage3(c)
        norm_chunk(full2, gain2, nrm, c)

    def up(c):
        ffo[...] = lax.dot_general(nrm[...], wff[...], NT, preferred_element_type=F32)

    def act(c):
        base = c * CH

        def body(i, carry):
            r = pl.multiple_of(i * 16, 16)
            rows = pl.ds(r, 16)
            hid[pl.ds(base + r, 16), :] = (jax.nn.silu(ffo[rows, :FFL]) * ffo[rows, FP:]).astype(BF16)
            return carry

        lax.fori_loop(0, CH // 16, body, 0, unroll=2)

    def down(c):
        rows = pl.ds(c * CH, CH)
        for j in range(8):
            part2[j // 2, j % 2, rows, :] = jnp.dot(
                hid[rows, :], wd[:, j * CB : (j + 1) * CB], preferred_element_type=F32
            ).astype(BF16)
        sum2.stage0(c)

    def finish(c):
        rows = pl.ds(c * CH, CH)
        layer_out = (full2[tp, rows, :].astype(F32) + sum2.stage3(c)).astype(BF16)
        ordered = jnp.dot(perm[...], layer_out, preferred_element_type=F32).astype(BF16)
        for s in range(SEQS):
            out[pl.ds(s * LEN + c * STEPS, STEPS), :] = ordered[s * STEPS : (s + 1) * STEPS]

    g_wgi.own()
    spread1.stage0(0)
    local[3].wait()
    g_wo.own()
    spread1.stage0(1)
    spread1.stage0(3)
    spread1.stage0(2)
    small_operands()
    g_wgi.near()
    g_wo.near()
    spread1.stage1(3)
    g_wgi.far()
    spread1.stage1(1)
    g_wgi.relay(2)
    g_wo.far()
    spread1.stage1(2)
    g_wgi.relay(0)
    spread1.stage1(0)
    g_wgi.relay(1)
    spread1.stage2(3)
    g_wgi.relay(3)
    g_wo.relay(3)
    spread1.stage2(2)
    g_wo.relay(2)
    g_wo.relay(0)
    g_wo.relay(1)
    spread1.stage2(1)
    local[4].wait()
    local[5].wait()
    g_wff.own()
    spread1.stage2(0)
    norm1(0)
    g_wgi.done()
    project(0)
    scan(0)
    g_wo.done()
    mix_out(0)
    norm1(1)
    project(1)
    sum1.stage1(0)
    g_wff.near()
    scan(1)
    mix_out(1)
    sum1.stage1(1)
    sum1.stage2(0)
    g_wff.relay(0)
    g_wff.far()
    local[6].wait()
    g_wd.own()
    norm1(2)
    project(2)
    sum1.stage2(1)
    scan(2)
    mix_out(2)
    settle(0)
    norm1(3)
    project(3)
    sum1.stage1(2)
    settle(1)
    g_wff.relay(2)
    scan(3)
    mix_out(3)
    g_wff.relay(1)
    sum1.stage2(2)
    sum1.stage1(3)
    g_wff.relay(3)
    spread1.drain()
    g_wd.near()
    spread2.stage1(0)
    spread2.stage1(1)
    g_wgi.drain()
    g_wo.drain()
    settle(2)
    sum1.stage2(3)
    spread2.stage2(0)
    norm2(0)
    spread2.stage2(1)
    g_wff.done()
    up(0)
    spread2.stage1(2)
    g_wd.far()
    act(0)
    norm2(1)
    g_wd.relay(1)
    up(1)
    g_wd.relay(2)
    settle(3)
    spread2.stage2(2)
    act(1)
    g_wd.relay(0)
    g_wd.relay(3)
    norm2(2)
    up(2)
    act(2)
    spread2.stage1(3)
    g_wd.done()
    down(0)
    down(1)
    down(2)
    sum2.stage1(0)
    sum2.stage1(1)
    sum2.stage1(2)
    spread2.stage2(3)
    g_wff.drain()
    sum2.stage2(0)
    norm2(3)
    up(3)
    sum2.stage2(2)
    act(3)
    down(3)
    perm[...] = order((CH, CH), "sequence")
    g_wd.drain()
    finish(0)
    sum2.stage1(3)
    sum2.stage2(1)
    sum1.drain(full1)
    finish(2)
    spread2.drain()
    sum2.stage2(3)
    finish(1)
    finish(3)

    sum2.drain(full2)


def layer(*operands):
    sums = [
        pltpu.VMEM((SIDE, 2, ROWS, CB), BF16),
        pltpu.VMEM((SIDE, ROWS, CB), BF16),
        pltpu.VMEM((SIDE, ROWS, CB), BF16),
        pltpu.VMEM((2, CHUNKS, HALF, CB), BF16),
        pltpu.VMEM((2, ROWS, CB), BF16),
    ]
    return pl.pallas_call(
        kernel,
        out_shape=jax.ShapeDtypeStruct((ROWS, CB), BF16),
        in_specs=[pl.BlockSpec(memory_space=pl.ANY)] * len(operands),
        out_specs=pl.BlockSpec(memory_space=pltpu.VMEM),
        scratch_shapes=[
            pltpu.VMEM((8, ROWS, CB), BF16),
            pltpu.VMEM((8, ROWS, CB), BF16),
            pltpu.VMEM((2 * RP, 2048), BF16),
            pltpu.VMEM((RP, 2048), BF16),
            pltpu.VMEM((FP + FFL, 2048), BF16),
            pltpu.VMEM((FFL, 2048), BF16),
            *sums,
            *sums,
            pltpu.VMEM((ROWS, CB), BF16),
            pltpu.VMEM((R, R), BF16),
            pltpu.VMEM((R, R), BF16),
            pltpu.VMEM((4, R), F32),
            pltpu.VMEM((R,), F32),
            pltpu.VMEM((SEQS, LEN), F32),
            pltpu.VMEM((16, 128), F32),
            pltpu.VMEM((16, 128), F32),
            pltpu.VMEM((RP, 2 * RP), BF16),
            pltpu.VMEM((8, RP), F32),
            pltpu.VMEM((ROWS, 128), F32),
            pltpu.VMEM((CH, CH), BF16),
            pltpu.VMEM((24 + ROWS, RP), F32),
            pltpu.VMEM((CH, RP), F32),
            pltpu.VMEM((CH, RP), BF16),
            pltpu.VMEM((CH, 2 * RP), F32),
            pltpu.VMEM((CH, RP), BF16),
            pltpu.VMEM((CH, 2048), BF16),
            pltpu.VMEM((CH, FP + FFL), F32),
            pltpu.VMEM((ROWS, FFL), BF16),
            pltpu.VMEM((SEQS, RP), F32),
            pltpu.SemaphoreType.DMA((14,)),
            pltpu.SemaphoreType.DMA((4,)),
            pltpu.SemaphoreType.DMA((4, 7)),
            pltpu.SemaphoreType.DMA((2,)),
            pltpu.SemaphoreType.DMA((2, 3, CHUNKS)),
            pltpu.SemaphoreType.DMA((2,)),
            pltpu.SemaphoreType.DMA((2, 3, CHUNKS)),
        ],
        compiler_params=pltpu.CompilerParams(
            collective_id=0, has_side_effects=True, vmem_limit_bytes=66_000_000
        ),
    )(*operands)


def shards(
    tokens,
    recurrence_norm_gain,
    output_gate_weight,
    recurrence_input_weight,
    convolution_taps,
    recurrence_gate_weight,
    input_gate_weight,
    base_decay_logit,
    token_log_decay,
    recurrence_output_weight,
    feedforward_norm_gain,
    feedforward_gate_weight,
    feedforward_up_weight,
    feedforward_down_weight,
):
    return layer(
        output_gate_weight.T,
        recurrence_input_weight.T,
        tokens,
        recurrence_output_weight,
        feedforward_gate_weight.T,
        feedforward_up_weight.T,
        feedforward_down_weight,
        recurrence_gate_weight.reshape(R, R),
        input_gate_weight.reshape(R, R),
        convolution_taps,
        base_decay_logit,
        token_log_decay.reshape(SEQS, LEN),
        recurrence_norm_gain.reshape(16, 128),
        feedforward_norm_gain.reshape(16, 128),
    )


def solution(mesh):
    in_specs = (
        P("fs", "tp"),
        P(),
        P("fs", "tp"),
        P("fs", "tp"),
        P(None, "tp"),
        P("tp", None, None),
        P("tp", None, None),
        P("tp"),
        P("fs"),
        P("tp", "fs"),
        P(),
        P("fs", "tp"),
        P("fs", "tp"),
        P("tp", "fs"),
    )
    return jax.shard_map(shards, mesh=mesh, in_specs=in_specs, out_specs=P("fs", "tp"), check_vma=False)
```

```python
import jax
import jax.numpy as jnp
from jax import lax
from jax.experimental import pallas as pl
from jax.experimental.pallas import tpu as pltpu
from jax.sharding import PartitionSpec as P

MESH = pl.DeviceIdType.MESH
F32 = jnp.float32
BF16 = jnp.bfloat16

LEN = 128
EPSILON = 1e-06
GATE_EXPONENT = 8.0

SIDE = 4
CHUNKS = 4
ROWS = 1024
CH = ROWS // CHUNKS
HALF = CH // 2
STEPS = LEN // CHUNKS
SEQS = 8
R = 352
RP = 384
FFL = 704
FP = 768
CB = 256
NT = (((1,), (1,)), ((), ()))

WGI_ROWS = (((0, 176), (176, 176)), ((RP, 176), (RP + 176, 176)))
WO_ROWS = (((0, 96), (96, 80)), ((176, 96), (272, 80)))
WFF_ROWS = (((0, 352), (352, 352)), ((FP, 352), (FP + 352, 352)))
WD_ROWS = (((0, 176), (176, 176)), ((352, 176), (528, 176)))


class Gather:
    def __init__(self, buf, rows, send, recv, pos, dev):
        self.buf, self.rows, self.send, self.recv, self.dev = buf, rows, send, recv, dev
        self.axes = (("x", "z"), ("z", "x"))
        self.pos = pos

    def block(self, part, i1, i2, half=None):
        z, x = (i2, i1) if part == 0 else (i1, i2)
        lo, hi = self.rows[part]
        span = pl.ds(lo[0], lo[1] + hi[1]) if half is None else pl.ds(*(lo, hi)[half])
        return self.buf.at[span, pl.ds(pl.multiple_of((z * SIDE + x) * 128, 128), 128)]

    def group(self, k):
        if k < 4:
            return k // 2
        return 6 if (k - 4) % 4 >= 2 else 2 + (k - 4) // 4

    def copy(self, view, part, k, to):
        return pltpu.make_async_remote_copy(
            src_ref=view,
            dst_ref=view,
            send_sem=self.send,
            recv_sem=self.recv.at[self.group(k)],
            device_id=to,
            device_id_type=MESH,
        )

    def blocks(self, count, group):
        (lo, hi), _ = self.rows
        view = self.buf.at[pl.ds(0, 2 * (lo[1] + hi[1])), pl.ds(0, 128 * count)]
        return pltpu.make_async_remote_copy(
            src_ref=view,
            dst_ref=view,
            send_sem=self.send,
            recv_sem=self.recv.at[group],
            device_id=self.dev["x"][0],
            device_id_type=MESH,
        )

    def places(self, part):
        a1, a2 = self.axes[part]
        (m1, i1, p1), (m2, i2, p2) = self.pos[a1], self.pos[a2]
        far1, far2 = lax.rem(i1 + 2, SIDE), lax.rem(i2 + 2, SIDE)
        return (i1, m1, p1, far1), (i2, m2, p2, far2), self.dev[a1], self.dev[a2]

    def onto_second(self, part, q):
        first, second, _, dev2 = self.places(part)
        view = self.block(part, first[q], second[0])
        self.copy(view, part, 4 + 4 * q, dev2[1]).start()
        self.copy(view, part, 5 + 4 * q, dev2[0]).start()

    def own(self):
        for part in (0, 1):
            first, second, dev1, _ = self.places(part)
            view = self.block(part, first[0], second[0])
            self.copy(view, part, 0, dev1[1]).start()
            self.copy(view, part, 1, dev1[0]).start()
        for part in (0, 1):
            self.onto_second(part, 0)

    def near(self):
        self.blocks(2, 0).wait_recv()
        for part in (0, 1):
            first, second, dev1, _ = self.places(part)
            self.copy(self.block(part, first[1], second[0], 0), part, 2, dev1[1]).start()
            self.copy(self.block(part, first[2], second[0], 1), part, 3, dev1[0]).start()
        for part in (0, 1):
            self.onto_second(part, 1)
            self.onto_second(part, 2)

    def far(self):
        self.blocks(1, 1).wait_recv()
        for part in (0, 1):
            self.onto_second(part, 3)

    def relay(self, q):
        self.blocks(2, 2 + q).wait_recv()
        for part in (0, 1):
            first, second, _, dev2 = self.places(part)
            self.copy(self.block(part, first[q], second[1], 0), part, 6 + 4 * q, dev2[1]).start()
            self.copy(self.block(part, first[q], second[2], 1), part, 7 + 4 * q, dev2[0]).start()

    def done(self):
        self.blocks(4, 6).wait_recv()

    def drain(self):
        self.blocks(15, 0).wait_send()


class Spread:
    def __init__(self, buf, send, recv, y, core, dev):
        self.buf, self.send, self.recv, self.dev = buf, send, recv, dev
        (ym, yy, yp), far = y, lax.rem(y[1] + 2, SIDE)
        other = 1 - core
        self.own, self.minus, self.plus, self.far = (2 * v + core for v in (yy, ym, yp, far))
        self.others = [2 * v + other for v in (yy, ym, yp, far)]

    def view(self, block, c, half=None):
        if half is None:
            return self.buf.at[block, pl.ds(c * CH, CH), :]
        return self.buf.at[block, pl.ds(c * CH + half * HALF, HALF), :]

    def copy(self, view, k, c, to):
        return pltpu.make_async_remote_copy(
            src_ref=view,
            dst_ref=view,
            send_sem=self.send,
            recv_sem=self.recv.at[(0, 0, 2, 1, 1, 2, 2, 2)[k], c],
            device_id=to,
            device_id_type=MESH,
        )

    def arrived(self, count, group, c):
        view = self.buf.at[pl.ds(0, count), pl.ds(c * CH, CH), :]
        pltpu.make_async_remote_copy(
            src_ref=view,
            dst_ref=view,
            send_sem=self.send,
            recv_sem=self.recv.at[group, c],
            device_id=self.dev["core"],
            device_id_type=MESH,
        ).wait_recv()

    def stage0(self, c):
        view = self.view(self.own, c)
        self.copy(view, 0, c, self.dev["y"][1]).start()
        self.copy(view, 1, c, self.dev["y"][0]).start()
        self.copy(view, 2, c, self.dev["core"]).start()

    def stage1(self, c):
        self.arrived(2, 0, c)
        self.copy(self.view(self.minus, c, 0), 3, c, self.dev["y"][1]).start()
        self.copy(self.view(self.minus, c), 5, c, self.dev["core"]).start()
        self.copy(self.view(self.plus, c, 1), 4, c, self.dev["y"][0]).start()
        self.copy(self.view(self.plus, c), 6, c, self.dev["core"]).start()

    def stage2(self, c):
        self.arrived(1, 1, c)
        self.copy(self.view(self.far, c), 7, c, self.dev["core"]).start()

    def stage3(self, c):
        self.arrived(4, 2, c)

    def drain(self):
        view = self.buf.at[pl.ds(0, 7)]
        pltpu.make_async_remote_copy(
            src_ref=view,
            dst_ref=view,
            send_sem=self.send,
            recv_sem=self.recv.at[0, 0],
            device_id=self.dev["core"],
            device_id_type=MESH,
        ).wait_send()


class Sum:
    def __init__(self, part, took, total, halves, finals, send, recv, y, core, dev):
        self.part, self.took, self.total = part, took, total
        self.halves, self.finals, self.send, self.recv, self.dev = halves, finals, send, recv, dev
        self.minus, self.own, self.plus = y
        self.far = lax.rem(y[1] + 2, SIDE)
        self.core = core

    def rows(self, c):
        return pl.ds(c * CH, CH)

    def half(self, c, h):
        return pl.ds(c * CH + h * HALF, HALF)

    def parts(self, k, c):
        if k == 0:
            return self.part.at[:, 1 - self.core, self.rows(c), :], self.took.at[:, self.rows(c), :], self.dev["core"]
        if k <= 2:
            return self.total.at[self.far, self.half(c, k - 1), :], self.halves.at[k - 1, c], self.dev["y"][2 - k]
        to = self.plus if k == 3 else self.minus
        return self.total.at[to, self.rows(c), :], self.finals.at[k - 3, self.rows(c), :], self.dev["y"][4 - k]

    def copy(self, k, c):
        src, dst, to = self.parts(k, c)
        return pltpu.make_async_remote_copy(
            src_ref=src,
            dst_ref=dst,
            send_sem=self.send,
            recv_sem=self.recv.at[(k + 1) // 2, c],
            device_id=to,
            device_id_type=MESH,
        )

    def arrived(self, view, group, c):
        pltpu.make_async_remote_copy(
            src_ref=view,
            dst_ref=view,
            send_sem=self.send,
            recv_sem=self.recv.at[group, c],
            device_id=self.dev["core"],
            device_id_type=MESH,
        ).wait_recv()

    def stage0(self, c):
        self.copy(0, c).start()

    def stage1(self, c):
        self.copy(0, c).wait_recv()
        rows = self.rows(c)

        def add(target):
            self.total[target, rows, :] = (
                self.part[target, self.core, rows, :].astype(F32) + self.took[target, rows, :].astype(F32)
            ).astype(BF16)

        add(self.far)
        add(self.plus)
        self.copy(1, c).start()
        self.copy(2, c).start()
        add(self.minus)
        add(self.own)

    def stage2(self, c):
        self.arrived(self.halves.at[:, c], 1, c)
        for h, target in ((0, self.plus), (1, self.minus)):
            rows = self.half(c, h)
            self.total[target, rows, :] = (
                self.total[target, rows, :].astype(F32) + self.halves[h, c].astype(F32)
            ).astype(BF16)
        self.copy(3, c).start()
        self.copy(4, c).start()

    def stage3(self, c):
        rows = self.rows(c)
        self.arrived(self.finals.at[:, rows, :], 2, c)
        return (
            self.total[self.own, rows, :].astype(F32)
            + self.finals[0, rows, :].astype(F32)
            + self.finals[1, rows, :].astype(F32)
        )

    def drain(self, like):
        view = like.at[pl.ds(0, 7)]
        pltpu.make_async_remote_copy(
            src_ref=view,
            dst_ref=view,
            send_sem=self.send,
            recv_sem=self.recv.at[0, 0],
            device_id=self.dev["core"],
            device_id_type=MESH,
        ).wait_send()


def norm_chunk(full, gain, out, c):
    step = 16

    def body(i, carry):
        rows = pl.ds(pl.multiple_of(c * CH + i * step, step), step)
        here = pl.ds(pl.multiple_of(i * step, step), step)
        total = jnp.zeros((step, CB), F32)
        for b in range(8):
            v = full[b, rows, :].astype(F32)
            total = total + v * v
        scale = lax.rsqrt(jnp.sum(total, axis=1, keepdims=True) * (1.0 / 2048.0) + EPSILON)
        for b in range(8):
            v = full[b, rows, :].astype(F32) * scale
            for s in range(2):
                g = gain[2 * b + s : 2 * b + s + 1, :]
                lo = b * CB + s * 128
                out[here, lo : lo + 128] = (v[:, s * 128 : s * 128 + 128] * g).astype(BF16)
        return carry

    lax.fori_loop(0, CH // step, body, 0, unroll=4)


def order(shape, major):
    to = lax.broadcasted_iota(jnp.int32, shape, 0)
    source = lax.broadcasted_iota(jnp.int32, shape, 1)
    if major == "time":
        wanted = lax.rem(to, SEQS) * STEPS + to // SEQS
    else:
        wanted = lax.rem(to, STEPS) * SEQS + to // STEPS
    return jnp.where(source == wanted, 1.0, 0.0).astype(BF16)


def kernel(
    wg_hbm, wi_hbm, tok_hbm, wo_hbm, wfg_hbm, wfu_hbm, wd_hbm,
    gr_hbm, gi_hbm, taps_hbm, base_hbm, ld_hbm, gain1_hbm, gain2_hbm,
    out,
    full1, full2, wgi, wo, wff, wd,
    part1, took1, total1, halves1, finals1,
    part2, took2, total2, halves2, finals2,
    tokv, grv, giv, tapsv, basev, ldv, gain1, gain2,
    gm, small, ldb, perm,
    feat, proj, mixed, gl, carried, nrm, ffo, hid, state,
    local_sem, w_send, w_recv, a_send, a_recv, s_send, s_recv,
):
    fs, tp = lax.axis_index("fs"), lax.axis_index("tp")
    iz, ix = fs // SIDE, lax.rem(fs, SIDE)
    iy, core = tp // 2, lax.rem(tp, 2)

    def ring(i):
        return lax.rem(i + SIDE - 1, SIDE), i, lax.rem(i + 1, SIDE)

    pos = {"x": ring(ix), "z": ring(iz)}
    y = ring(iy)
    dev = {
        "x": tuple({"fs": iz * SIDE + pos["x"][k]} for k in (0, 2)),
        "z": tuple({"fs": pos["z"][k] * SIDE + ix} for k in (0, 2)),
        "y": tuple({"tp": 2 * y[k] + core} for k in (0, 2)),
        "core": {"tp": 2 * iy + 1 - core},
    }

    barrier = pltpu.get_barrier_semaphore()
    for to in (*dev["x"], *dev["z"], *dev["y"], dev["core"]):
        pl.semaphore_signal(barrier, inc=1, device_id=to, device_id_type=MESH)

    cols = pl.ds(pl.multiple_of(fs * 128, 128), 128)
    local = [
        pltpu.make_async_copy(src, dst, local_sem.at[n])
        for n, (src, dst) in enumerate(
            (
                (wg_hbm, wgi.at[pl.ds(0, R), cols]),
                (wi_hbm, wgi.at[pl.ds(RP, R), cols]),
                (tok_hbm, tokv),
                (wo_hbm, wo.at[pl.ds(0, R), cols]),
                (wfg_hbm, wff.at[pl.ds(0, FFL), cols]),
                (wfu_hbm, wff.at[pl.ds(FP, FFL), cols]),
                (wd_hbm, wd.at[:, cols]),
                (gr_hbm, grv),
                (gi_hbm, giv),
                (taps_hbm, tapsv),
                (base_hbm, basev),
                (ld_hbm, ldv),
                (gain1_hbm, gain1),
                (gain2_hbm, gain2),
            )
        )
    ]
    for copy in local:
        copy.start()
    wgi[R:RP, :] = jnp.zeros((RP - R, 2048), BF16)
    wgi[RP + R :, :] = jnp.zeros((RP - R, 2048), BF16)
    wo[R:RP, :] = jnp.zeros((RP - R, 2048), BF16)
    wff[FFL:FP, :] = jnp.zeros((FP - FFL, 2048), BF16)
    perm[...] = order((CH, CH), "time")

    gathers = [
        Gather(buf, rows, w_send.at[m], w_recv.at[m], pos, dev)
        for m, (buf, rows) in enumerate(((wgi, WGI_ROWS), (wo, WO_ROWS), (wff, WFF_ROWS), (wd, WD_ROWS)))
    ]
    g_wgi, g_wo, g_wff, g_wd = gathers
    spread1 = Spread(full1, a_send.at[0], a_recv.at[0], y, core, dev)
    spread2 = Spread(full2, a_send.at[1], a_recv.at[1], y, core, dev)
    sum1 = Sum(part1, took1, total1, halves1, finals1, s_send.at[0], s_recv.at[0], y, core, dev)
    sum2 = Sum(part2, took2, total2, halves2, finals2, s_send.at[1], s_recv.at[1], y, core, dev)

    def reordered(c):
        pieces = [tokv[s * LEN + c * STEPS : s * LEN + (c + 1) * STEPS, :] for s in range(SEQS)]
        full1[tp, c * CH : (c + 1) * CH, :] = jnp.dot(
            perm[...], jnp.concatenate(pieces, axis=0), preferred_element_type=F32
        ).astype(BF16)

    local[2].wait()
    for c in range(CHUNKS):
        reordered(c)
    local[0].wait()
    local[1].wait()
    pl.semaphore_wait(barrier, 7)

    def small_operands():
        for n in range(7, 14):
            local[n].wait()
        gm[...] = jnp.zeros_like(gm)
        gm[0:R, 0:R] = grv[...]
        gm[0:R, RP : RP + R] = giv[...]
        small[...] = jnp.zeros_like(small)
        small[0:4, 0:R] = tapsv[...]
        small[4:5, 0:R] = -GATE_EXPONENT * jax.nn.softplus(-basev[...].reshape(1, R))
        for t in range(LEN):
            ldb[8 * t : 8 * t + 8, :] = jnp.broadcast_to(ldv[:, t : t + 1], (SEQS, 128))
        feat[0:24, :] = jnp.zeros((24, RP), F32)
        state[...] = jnp.zeros_like(state)

    def norm1(c):
        spread1.stage3(c)
        norm_chunk(full1, gain1, nrm, c)

    def project(c):
        base = c * CH
        projected = lax.dot_general(nrm[...], wgi[...], NT, preferred_element_type=F32)
        proj[...] = projected[:, :RP]
        feat[pl.ds(base + 24, CH), :] = projected[:, RP:].astype(BF16).astype(F32)

    def scan(c):
        base = c * CH

        def taps(i, carry):
            r = pl.multiple_of(i * 32, 32)
            summed = small[0:1, :] * feat[pl.ds(base + r, 32), :]
            for k in range(1, 4):
                summed = summed + small[k : k + 1, :] * feat[pl.ds(base + r + 8 * k, 32), :]
            mixed[pl.ds(r, 32), :] = summed.astype(BF16)
            return carry

        lax.fori_loop(0, CH // 32, taps, 0, unroll=2)
        gl[...] = jnp.dot(mixed[...], gm[...], preferred_element_type=F32)

        def steps(i, h):
            r = pl.multiple_of(i * 32, 32)
            rows = pl.ds(r, 32)
            recur = jax.nn.sigmoid(gl[rows, :RP])
            inject = jax.nn.sigmoid(gl[rows, RP:])
            struck = ldb[pl.ds(base + r, 32), :]
            log_decay = small[4:5, :] * recur + jnp.concatenate([struck] * 3, axis=1)
            decay = jnp.exp(log_decay)
            twice = 2.0 * log_decay
            near = -twice * (1.0 + twice * (0.5 + twice * (1.0 / 6.0 + twice * (1.0 / 24.0 + twice * (1.0 / 120.0)))))
            rest = jnp.where(twice > -0.1, near, 1.0 - decay * decay)
            driven = jnp.sqrt(rest) * (inject * mixed[rows, :].astype(F32))
            states = []
            for s in range(4):
                h = decay[8 * s : 8 * s + 8] * h + driven[8 * s : 8 * s + 8]
                states.append(h)
            carried[rows, :] = (jnp.concatenate(states, axis=0) * jax.nn.gelu(proj[rows, :])).astype(BF16)
            return h

        state[...] = lax.fori_loop(0, CH // 32, steps, state[...], unroll=2)

    def mix_out(c):
        rows = pl.ds(c * CH, CH)
        for j in range(8):
            part1[j // 2, j % 2, rows, :] = jnp.dot(
                carried[...], wo[:, j * CB : (j + 1) * CB], preferred_element_type=F32
            ).astype(BF16)
        sum1.stage0(c)

    def settle(c):
        rows = pl.ds(c * CH, CH)
        full2[tp, rows, :] = (full1[tp, rows, :].astype(F32) + sum1.stage3(c)).astype(BF16)
        spread2.stage0(c)

    def norm2(c):
        spread2.stage3(c)
        norm_chunk(full2, gain2, nrm, c)

    def up(c):
        ffo[...] = lax.dot_general(nrm[...], wff[...], NT, preferred_element_type=F32)

    def act(c):
        base = c * CH

        def body(i, carry):
            r = pl.multiple_of(i * 16, 16)
            rows = pl.ds(r, 16)
            hid[pl.ds(base + r, 16), :] = (jax.nn.silu(ffo[rows, :FFL]) * ffo[rows, FP:]).astype(BF16)
            return carry

        lax.fori_loop(0, CH // 16, body, 0, unroll=2)

    def down(c):
        rows = pl.ds(c * CH, CH)
        for j in range(8):
            part2[j // 2, j % 2, rows, :] = jnp.dot(
                hid[rows, :], wd[:, j * CB : (j + 1) * CB], preferred_element_type=F32
            ).astype(BF16)
        sum2.stage0(c)

    def finish(c):
        rows = pl.ds(c * CH, CH)
        layer_out = (full2[tp, rows, :].astype(F32) + sum2.stage3(c)).astype(BF16)
        ordered = jnp.dot(perm[...], layer_out, preferred_element_type=F32).astype(BF16)
        for s in range(SEQS):
            out[pl.ds(s * LEN + c * STEPS, STEPS), :] = ordered[s * STEPS : (s + 1) * STEPS]

    local[3].wait()
    g_wo.own()
    spread1.stage0(0)
    spread1.stage0(2)
    g_wgi.own()
    g_wo.near()
    spread1.stage0(1)
    small_operands()
    g_wgi.near()
    spread1.stage1(1)
    g_wo.far()
    spread1.stage1(0)
    spread1.stage0(3)
    g_wgi.far()
    g_wgi.relay(2)
    g_wgi.relay(0)
    spread1.stage1(2)
    spread1.stage2(1)
    g_wgi.relay(1)
    g_wgi.relay(3)
    g_wo.relay(1)
    g_wo.relay(2)
    g_wo.relay(3)
    spread1.stage2(0)
    g_wo.relay(0)
    spread1.stage1(3)
    local[6].wait()
    g_wd.own()
    norm1(0)
    local[4].wait()
    local[5].wait()
    g_wff.own()
    g_wgi.done()
    project(0)
    scan(0)
    g_wo.done()
    mix_out(0)
    norm1(1)
    project(1)
    sum1.stage1(0)
    scan(1)
    mix_out(1)
    sum1.stage1(1)
    spread1.stage2(2)
    sum1.stage2(0)
    g_wff.near()
    spread1.stage2(3)
    norm1(2)
    project(2)
    sum1.stage2(1)
    scan(2)
    mix_out(2)
    settle(0)
    norm1(3)
    sum1.stage1(2)
    project(3)
    scan(3)
    g_wff.far()
    settle(1)
    spread2.stage1(0)
    g_wff.relay(1)
    sum1.stage2(2)
    g_wff.relay(2)
    mix_out(3)
    g_wff.relay(3)
    g_wff.relay(0)
    spread1.drain()
    g_wd.near()
    sum1.stage1(3)
    spread2.stage1(1)
    g_wgi.drain()
    g_wo.drain()
    settle(2)
    spread2.stage2(0)
    norm2(0)
    sum1.stage2(3)
    spread2.stage2(1)
    g_wff.done()
    up(0)
    g_wd.far()
    act(0)
    spread2.stage1(2)
    g_wd.relay(0)
    norm2(1)
    g_wd.relay(1)
    settle(3)
    up(1)
    g_wd.relay(2)
    spread2.stage2(2)
    g_wd.relay(3)
    act(1)
    norm2(2)
    up(2)
    act(2)
    spread2.stage1(3)
    g_wd.done()
    down(0)
    down(1)
    sum2.stage1(0)
    down(2)
    sum2.stage1(1)
    spread2.stage2(3)
    sum2.stage1(2)
    norm2(3)
    g_wff.drain()
    sum2.stage2(0)
    up(3)
    act(3)
    sum2.stage2(1)
    down(3)
    sum2.stage1(3)
    sum2.stage2(2)
    spread2.drain()
    sum2.stage2(3)
    sum1.drain(full1)
    perm[...] = order((CH, CH), "sequence")
    finish(2)
    finish(1)
    g_wd.drain()
    finish(0)
    finish(3)

    sum2.drain(full2)


def layer(*operands):
    sums = [
        pltpu.VMEM((SIDE, 2, ROWS, CB), BF16),
        pltpu.VMEM((SIDE, ROWS, CB), BF16),
        pltpu.VMEM((SIDE, ROWS, CB), BF16),
        pltpu.VMEM((2, CHUNKS, HALF, CB), BF16),
        pltpu.VMEM((2, ROWS, CB), BF16),
    ]
    return pl.pallas_call(
        kernel,
        out_shape=jax.ShapeDtypeStruct((ROWS, CB), BF16),
        in_specs=[pl.BlockSpec(memory_space=pl.ANY)] * len(operands),
        out_specs=pl.BlockSpec(memory_space=pltpu.VMEM),
        scratch_shapes=[
            pltpu.VMEM((8, ROWS, CB), BF16),
            pltpu.VMEM((8, ROWS, CB), BF16),
            pltpu.VMEM((2 * RP, 2048), BF16),
            pltpu.VMEM((RP, 2048), BF16),
            pltpu.VMEM((FP + FFL, 2048), BF16),
            pltpu.VMEM((FFL, 2048), BF16),
            *sums,
            *sums,
            pltpu.VMEM((ROWS, CB), BF16),
            pltpu.VMEM((R, R), BF16),
            pltpu.VMEM((R, R), BF16),
            pltpu.VMEM((4, R), F32),
            pltpu.VMEM((R,), F32),
            pltpu.VMEM((SEQS, LEN), F32),
            pltpu.VMEM((16, 128), F32),
            pltpu.VMEM((16, 128), F32),
            pltpu.VMEM((RP, 2 * RP), BF16),
            pltpu.VMEM((8, RP), F32),
            pltpu.VMEM((ROWS, 128), F32),
            pltpu.VMEM((CH, CH), BF16),
            pltpu.VMEM((24 + ROWS, RP), F32),
            pltpu.VMEM((CH, RP), F32),
            pltpu.VMEM((CH, RP), BF16),
            pltpu.VMEM((CH, 2 * RP), F32),
            pltpu.VMEM((CH, RP), BF16),
            pltpu.VMEM((CH, 2048), BF16),
            pltpu.VMEM((CH, FP + FFL), F32),
            pltpu.VMEM((ROWS, FFL), BF16),
            pltpu.VMEM((SEQS, RP), F32),
            pltpu.SemaphoreType.DMA((14,)),
            pltpu.SemaphoreType.DMA((4,)),
            pltpu.SemaphoreType.DMA((4, 7)),
            pltpu.SemaphoreType.DMA((2,)),
            pltpu.SemaphoreType.DMA((2, 3, CHUNKS)),
            pltpu.SemaphoreType.DMA((2,)),
            pltpu.SemaphoreType.DMA((2, 3, CHUNKS)),
        ],
        compiler_params=pltpu.CompilerParams(
            collective_id=0, has_side_effects=True, vmem_limit_bytes=66_000_000
        ),
    )(*operands)


def shards(
    tokens,
    recurrence_norm_gain,
    output_gate_weight,
    recurrence_input_weight,
    convolution_taps,
    recurrence_gate_weight,
    input_gate_weight,
    base_decay_logit,
    token_log_decay,
    recurrence_output_weight,
    feedforward_norm_gain,
    feedforward_gate_weight,
    feedforward_up_weight,
    feedforward_down_weight,
):
    return layer(
        output_gate_weight.T,
        recurrence_input_weight.T,
        tokens,
        recurrence_output_weight,
        feedforward_gate_weight.T,
        feedforward_up_weight.T,
        feedforward_down_weight,
        recurrence_gate_weight.reshape(R, R),
        input_gate_weight.reshape(R, R),
        convolution_taps,
        base_decay_logit,
        token_log_decay.reshape(SEQS, LEN),
        recurrence_norm_gain.reshape(16, 128),
        feedforward_norm_gain.reshape(16, 128),
    )


def solution(mesh):
    in_specs = (
        P("fs", "tp"),
        P(),
        P("fs", "tp"),
        P("fs", "tp"),
        P(None, "tp"),
        P("tp", None, None),
        P("tp", None, None),
        P("tp"),
        P("fs"),
        P("tp", "fs"),
        P(),
        P("fs", "tp"),
        P("fs", "tp"),
        P("tp", "fs"),
    )
    return jax.shard_map(shards, mesh=mesh, in_specs=in_specs, out_specs=P("fs", "tp"), check_vma=False)
```

```python
import jax
import jax.numpy as jnp
from jax import lax
from jax.experimental import pallas as pl
from jax.experimental.pallas import tpu as pltpu
from jax.sharding import PartitionSpec as P

MESH = pl.DeviceIdType.MESH
F32 = jnp.float32
BF16 = jnp.bfloat16

LEN = 128
EPSILON = 1e-06
GATE_EXPONENT = 8.0

SIDE = 4
CHUNKS = 4
ROWS = 1024
CH = ROWS // CHUNKS
HALF = CH // 2
STEPS = LEN // CHUNKS
SEQS = 8
R = 352
RP = 384
FFL = 704
FP = 768
CB = 256
NT = (((1,), (1,)), ((), ()))

WGI_ROWS = (((0, 176), (176, 176)), ((RP, 176), (RP + 176, 176)))
WO_ROWS = (((0, 96), (96, 80)), ((176, 96), (272, 80)))
WFF_ROWS = (((0, 352), (352, 352)), ((FP, 352), (FP + 352, 352)))
WD_ROWS = (((0, 176), (176, 176)), ((352, 176), (528, 176)))


class Gather:
    def __init__(self, buf, rows, send, recv, pos, dev):
        self.buf, self.rows, self.send, self.recv, self.dev = buf, rows, send, recv, dev
        self.axes = (("x", "z"), ("z", "x"))
        self.pos = pos

    def block(self, part, i1, i2, half=None):
        z, x = (i2, i1) if part == 0 else (i1, i2)
        lo, hi = self.rows[part]
        span = pl.ds(lo[0], lo[1] + hi[1]) if half is None else pl.ds(*(lo, hi)[half])
        return self.buf.at[span, pl.ds(pl.multiple_of((z * SIDE + x) * 128, 128), 128)]

    def group(self, k):
        if k < 4:
            return k // 2
        return 6 if (k - 4) % 4 >= 2 else 2 + (k - 4) // 4

    def copy(self, view, part, k, to):
        return pltpu.make_async_remote_copy(
            src_ref=view,
            dst_ref=view,
            send_sem=self.send,
            recv_sem=self.recv.at[self.group(k)],
            device_id=to,
            device_id_type=MESH,
        )

    def blocks(self, count, group):
        (lo, hi), _ = self.rows
        view = self.buf.at[pl.ds(0, 2 * (lo[1] + hi[1])), pl.ds(0, 128 * count)]
        return pltpu.make_async_remote_copy(
            src_ref=view,
            dst_ref=view,
            send_sem=self.send,
            recv_sem=self.recv.at[group],
            device_id=self.dev["x"][0],
            device_id_type=MESH,
        )

    def places(self, part):
        a1, a2 = self.axes[part]
        (m1, i1, p1), (m2, i2, p2) = self.pos[a1], self.pos[a2]
        far1, far2 = lax.rem(i1 + 2, SIDE), lax.rem(i2 + 2, SIDE)
        return (i1, m1, p1, far1), (i2, m2, p2, far2), self.dev[a1], self.dev[a2]

    def onto_second(self, part, q):
        first, second, _, dev2 = self.places(part)
        view = self.block(part, first[q], second[0])
        self.copy(view, part, 4 + 4 * q, dev2[1]).start()
        self.copy(view, part, 5 + 4 * q, dev2[0]).start()

    def own(self):
        for part in (0, 1):
            first, second, dev1, _ = self.places(part)
            view = self.block(part, first[0], second[0])
            self.copy(view, part, 0, dev1[1]).start()
            self.copy(view, part, 1, dev1[0]).start()
        for part in (0, 1):
            self.onto_second(part, 0)

    def near(self):
        self.blocks(2, 0).wait_recv()
        for part in (0, 1):
            first, second, dev1, _ = self.places(part)
            self.copy(self.block(part, first[1], second[0], 0), part, 2, dev1[1]).start()
            self.copy(self.block(part, first[2], second[0], 1), part, 3, dev1[0]).start()
        for part in (0, 1):
            self.onto_second(part, 1)
            self.onto_second(part, 2)

    def far(self):
        self.blocks(1, 1).wait_recv()
        for part in (0, 1):
            self.onto_second(part, 3)

    def relay(self, q):
        self.blocks(2, 2 + q).wait_recv()
        for part in (0, 1):
            first, second, _, dev2 = self.places(part)
            self.copy(self.block(part, first[q], second[1], 0), part, 6 + 4 * q, dev2[1]).start()
            self.copy(self.block(part, first[q], second[2], 1), part, 7 + 4 * q, dev2[0]).start()

    def done(self):
        self.blocks(4, 6).wait_recv()

    def drain(self):
        self.blocks(15, 0).wait_send()


class Spread:
    def __init__(self, buf, send, recv, y, core, dev):
        self.buf, self.send, self.recv, self.dev = buf, send, recv, dev
        (ym, yy, yp), far = y, lax.rem(y[1] + 2, SIDE)
        other = 1 - core
        self.own, self.minus, self.plus, self.far = (2 * v + core for v in (yy, ym, yp, far))
        self.others = [2 * v + other for v in (yy, ym, yp, far)]

    def view(self, block, c, half=None):
        if half is None:
            return self.buf.at[block, pl.ds(c * CH, CH), :]
        return self.buf.at[block, pl.ds(c * CH + half * HALF, HALF), :]

    def copy(self, view, k, c, to):
        return pltpu.make_async_remote_copy(
            src_ref=view,
            dst_ref=view,
            send_sem=self.send,
            recv_sem=self.recv.at[(0, 0, 2, 1, 1, 2, 2, 2)[k], c],
            device_id=to,
            device_id_type=MESH,
        )

    def arrived(self, count, group, c):
        view = self.buf.at[pl.ds(0, count), pl.ds(c * CH, CH), :]
        pltpu.make_async_remote_copy(
            src_ref=view,
            dst_ref=view,
            send_sem=self.send,
            recv_sem=self.recv.at[group, c],
            device_id=self.dev["core"],
            device_id_type=MESH,
        ).wait_recv()

    def stage0(self, c):
        view = self.view(self.own, c)
        self.copy(view, 0, c, self.dev["y"][1]).start()
        self.copy(view, 1, c, self.dev["y"][0]).start()
        self.copy(view, 2, c, self.dev["core"]).start()

    def stage1(self, c):
        self.arrived(2, 0, c)
        self.copy(self.view(self.minus, c, 0), 3, c, self.dev["y"][1]).start()
        self.copy(self.view(self.minus, c), 5, c, self.dev["core"]).start()
        self.copy(self.view(self.plus, c, 1), 4, c, self.dev["y"][0]).start()
        self.copy(self.view(self.plus, c), 6, c, self.dev["core"]).start()

    def stage2(self, c):
        self.arrived(1, 1, c)
        self.copy(self.view(self.far, c), 7, c, self.dev["core"]).start()

    def stage3(self, c):
        self.arrived(4, 2, c)

    def drain(self):
        view = self.buf.at[pl.ds(0, 7)]
        pltpu.make_async_remote_copy(
            src_ref=view,
            dst_ref=view,
            send_sem=self.send,
            recv_sem=self.recv.at[0, 0],
            device_id=self.dev["core"],
            device_id_type=MESH,
        ).wait_send()


class Sum:
    def __init__(self, part, took, total, halves, finals, send, recv, y, core, dev):
        self.part, self.took, self.total = part, took, total
        self.halves, self.finals, self.send, self.recv, self.dev = halves, finals, send, recv, dev
        self.minus, self.own, self.plus = y
        self.far = lax.rem(y[1] + 2, SIDE)
        self.core = core

    def rows(self, c):
        return pl.ds(c * CH, CH)

    def half(self, c, h):
        return pl.ds(c * CH + h * HALF, HALF)

    def parts(self, k, c):
        if k == 0:
            return self.part.at[:, 1 - self.core, self.rows(c), :], self.took.at[:, self.rows(c), :], self.dev["core"]
        if k <= 2:
            return self.total.at[self.far, self.half(c, k - 1), :], self.halves.at[k - 1, c], self.dev["y"][2 - k]
        to = self.plus if k == 3 else self.minus
        return self.total.at[to, self.rows(c), :], self.finals.at[k - 3, self.rows(c), :], self.dev["y"][4 - k]

    def copy(self, k, c):
        src, dst, to = self.parts(k, c)
        return pltpu.make_async_remote_copy(
            src_ref=src,
            dst_ref=dst,
            send_sem=self.send,
            recv_sem=self.recv.at[(k + 1) // 2, c],
            device_id=to,
            device_id_type=MESH,
        )

    def arrived(self, view, group, c):
        pltpu.make_async_remote_copy(
            src_ref=view,
            dst_ref=view,
            send_sem=self.send,
            recv_sem=self.recv.at[group, c],
            device_id=self.dev["core"],
            device_id_type=MESH,
        ).wait_recv()

    def stage0(self, c):
        self.copy(0, c).start()

    def stage1(self, c):
        self.copy(0, c).wait_recv()
        rows = self.rows(c)

        def add(target):
            self.total[target, rows, :] = (
                self.part[target, self.core, rows, :].astype(F32) + self.took[target, rows, :].astype(F32)
            ).astype(BF16)

        add(self.far)
        add(self.plus)
        self.copy(1, c).start()
        self.copy(2, c).start()
        add(self.minus)
        add(self.own)

    def stage2(self, c):
        self.arrived(self.halves.at[:, c], 1, c)
        for h, target in ((0, self.plus), (1, self.minus)):
            rows = self.half(c, h)
            self.total[target, rows, :] = (
                self.total[target, rows, :].astype(F32) + self.halves[h, c].astype(F32)
            ).astype(BF16)
        self.copy(3, c).start()
        self.copy(4, c).start()

    def stage3(self, c):
        rows = self.rows(c)
        self.arrived(self.finals.at[:, rows, :], 2, c)
        return (
            self.total[self.own, rows, :].astype(F32)
            + self.finals[0, rows, :].astype(F32)
            + self.finals[1, rows, :].astype(F32)
        )

    def drain(self, like):
        view = like.at[pl.ds(0, 7)]
        pltpu.make_async_remote_copy(
            src_ref=view,
            dst_ref=view,
            send_sem=self.send,
            recv_sem=self.recv.at[0, 0],
            device_id=self.dev["core"],
            device_id_type=MESH,
        ).wait_send()


def norm_chunk(full, gain, out, c):
    step = 16

    def body(i, carry):
        rows = pl.ds(pl.multiple_of(c * CH + i * step, step), step)
        here = pl.ds(pl.multiple_of(i * step, step), step)
        total = jnp.zeros((step, CB), F32)
        for b in range(8):
            v = full[b, rows, :].astype(F32)
            total = total + v * v
        scale = lax.rsqrt(jnp.sum(total, axis=1, keepdims=True) * (1.0 / 2048.0) + EPSILON)
        for b in range(8):
            v = full[b, rows, :].astype(F32) * scale
            for s in range(2):
                g = gain[2 * b + s : 2 * b + s + 1, :]
                lo = b * CB + s * 128
                out[here, lo : lo + 128] = (v[:, s * 128 : s * 128 + 128] * g).astype(BF16)
        return carry

    lax.fori_loop(0, CH // step, body, 0, unroll=4)


def order(shape, major):
    to = lax.broadcasted_iota(jnp.int32, shape, 0)
    source = lax.broadcasted_iota(jnp.int32, shape, 1)
    if major == "time":
        wanted = lax.rem(to, SEQS) * STEPS + to // SEQS
    else:
        wanted = lax.rem(to, STEPS) * SEQS + to // STEPS
    return jnp.where(source == wanted, 1.0, 0.0).astype(BF16)


def kernel(
    wg_hbm, wi_hbm, tok_hbm, wo_hbm, wfg_hbm, wfu_hbm, wd_hbm,
    gr_hbm, gi_hbm, taps_hbm, base_hbm, ld_hbm, gain1_hbm, gain2_hbm,
    out,
    full1, full2, wgi, wo, wff, wd,
    part1, took1, total1, halves1, finals1,
    part2, took2, total2, halves2, finals2,
    tokv, grv, giv, tapsv, basev, ldv, gain1, gain2,
    gm, small, ldb, perm,
    feat, proj, mixed, gl, carried, nrm, ffo, hid, state,
    local_sem, w_send, w_recv, a_send, a_recv, s_send, s_recv,
):
    fs, tp = lax.axis_index("fs"), lax.axis_index("tp")
    iz, ix = fs // SIDE, lax.rem(fs, SIDE)
    iy, core = tp // 2, lax.rem(tp, 2)

    def ring(i):
        return lax.rem(i + SIDE - 1, SIDE), i, lax.rem(i + 1, SIDE)

    pos = {"x": ring(ix), "z": ring(iz)}
    y = ring(iy)
    dev = {
        "x": tuple({"fs": iz * SIDE + pos["x"][k]} for k in (0, 2)),
        "z": tuple({"fs": pos["z"][k] * SIDE + ix} for k in (0, 2)),
        "y": tuple({"tp": 2 * y[k] + core} for k in (0, 2)),
        "core": {"tp": 2 * iy + 1 - core},
    }

    barrier = pltpu.get_barrier_semaphore()
    for to in (*dev["x"], *dev["z"], *dev["y"], dev["core"]):
        pl.semaphore_signal(barrier, inc=1, device_id=to, device_id_type=MESH)

    cols = pl.ds(pl.multiple_of(fs * 128, 128), 128)
    local = [
        pltpu.make_async_copy(src, dst, local_sem.at[n])
        for n, (src, dst) in enumerate(
            (
                (wg_hbm, wgi.at[pl.ds(0, R), cols]),
                (wi_hbm, wgi.at[pl.ds(RP, R), cols]),
                (tok_hbm, tokv),
                (wo_hbm, wo.at[pl.ds(0, R), cols]),
                (wfg_hbm, wff.at[pl.ds(0, FFL), cols]),
                (wfu_hbm, wff.at[pl.ds(FP, FFL), cols]),
                (wd_hbm, wd.at[:, cols]),
                (gr_hbm, grv),
                (gi_hbm, giv),
                (taps_hbm, tapsv),
                (base_hbm, basev),
                (ld_hbm, ldv),
                (gain1_hbm, gain1),
                (gain2_hbm, gain2),
            )
        )
    ]
    for copy in local:
        copy.start()
    wgi[R:RP, :] = jnp.zeros((RP - R, 2048), BF16)
    wgi[RP + R :, :] = jnp.zeros((RP - R, 2048), BF16)
    wo[R:RP, :] = jnp.zeros((RP - R, 2048), BF16)
    wff[FFL:FP, :] = jnp.zeros((FP - FFL, 2048), BF16)
    perm[...] = order((CH, CH), "time")

    gathers = [
        Gather(buf, rows, w_send.at[m], w_recv.at[m], pos, dev)
        for m, (buf, rows) in enumerate(((wgi, WGI_ROWS), (wo, WO_ROWS), (wff, WFF_ROWS), (wd, WD_ROWS)))
    ]
    g_wgi, g_wo, g_wff, g_wd = gathers
    spread1 = Spread(full1, a_send.at[0], a_recv.at[0], y, core, dev)
    spread2 = Spread(full2, a_send.at[1], a_recv.at[1], y, core, dev)
    sum1 = Sum(part1, took1, total1, halves1, finals1, s_send.at[0], s_recv.at[0], y, core, dev)
    sum2 = Sum(part2, took2, total2, halves2, finals2, s_send.at[1], s_recv.at[1], y, core, dev)

    def reordered(c):
        pieces = [tokv[s * LEN + c * STEPS : s * LEN + (c + 1) * STEPS, :] for s in range(SEQS)]
        full1[tp, c * CH : (c + 1) * CH, :] = jnp.dot(
            perm[...], jnp.concatenate(pieces, axis=0), preferred_element_type=F32
        ).astype(BF16)

    local[2].wait()
    for c in range(CHUNKS):
        reordered(c)
    local[0].wait()
    local[1].wait()
    pl.semaphore_wait(barrier, 7)

    def small_operands():
        for n in range(7, 14):
            local[n].wait()
        gm[...] = jnp.zeros_like(gm)
        gm[0:R, 0:R] = grv[...]
        gm[0:R, RP : RP + R] = giv[...]
        small[...] = jnp.zeros_like(small)
        small[0:4, 0:R] = tapsv[...]
        small[4:5, 0:R] = -GATE_EXPONENT * jax.nn.softplus(-basev[...].reshape(1, R))
        for t in range(LEN):
            ldb[8 * t : 8 * t + 8, :] = jnp.broadcast_to(ldv[:, t : t + 1], (SEQS, 128))
        feat[0:24, :] = jnp.zeros((24, RP), F32)
        state[...] = jnp.zeros_like(state)

    def norm1(c):
        spread1.stage3(c)
        norm_chunk(full1, gain1, nrm, c)

    def project(c):
        base = c * CH
        projected = lax.dot_general(nrm[...], wgi[...], NT, preferred_element_type=F32)
        proj[...] = projected[:, :RP]
        feat[pl.ds(base + 24, CH), :] = projected[:, RP:].astype(BF16).astype(F32)

    def scan(c):
        base = c * CH

        def taps(i, carry):
            r = pl.multiple_of(i * 32, 32)
            summed = small[0:1, :] * feat[pl.ds(base + r, 32), :]
            for k in range(1, 4):
                summed = summed + small[k : k + 1, :] * feat[pl.ds(base + r + 8 * k, 32), :]
            mixed[pl.ds(r, 32), :] = summed.astype(BF16)
            return carry

        lax.fori_loop(0, CH // 32, taps, 0, unroll=2)
        gl[...] = jnp.dot(mixed[...], gm[...], preferred_element_type=F32)

        def steps(i, h):
            r = pl.multiple_of(i * 32, 32)
            rows = pl.ds(r, 32)
            recur = jax.nn.sigmoid(gl[rows, :RP])
            inject = jax.nn.sigmoid(gl[rows, RP:])
            struck = ldb[pl.ds(base + r, 32), :]
            log_decay = small[4:5, :] * recur + jnp.concatenate([struck] * 3, axis=1)
            decay = jnp.exp(log_decay)
            twice = 2.0 * log_decay
            near = -twice * (1.0 + twice * (0.5 + twice * (1.0 / 6.0 + twice * (1.0 / 24.0 + twice * (1.0 / 120.0)))))
            rest = jnp.where(twice > -0.1, near, 1.0 - decay * decay)
            driven = jnp.sqrt(rest) * (inject * mixed[rows, :].astype(F32))
            states = []
            for s in range(4):
                h = decay[8 * s : 8 * s + 8] * h + driven[8 * s : 8 * s + 8]
                states.append(h)
            carried[rows, :] = (jnp.concatenate(states, axis=0) * jax.nn.gelu(proj[rows, :])).astype(BF16)
            return h

        state[...] = lax.fori_loop(0, CH // 32, steps, state[...], unroll=2)

    def mix_out(c):
        rows = pl.ds(c * CH, CH)
        for j in range(8):
            part1[j // 2, j % 2, rows, :] = jnp.dot(
                carried[...], wo[:, j * CB : (j + 1) * CB], preferred_element_type=F32
            ).astype(BF16)
        sum1.stage0(c)

    def settle(c):
        rows = pl.ds(c * CH, CH)
        full2[tp, rows, :] = (full1[tp, rows, :].astype(F32) + sum1.stage3(c)).astype(BF16)
        spread2.stage0(c)

    def norm2(c):
        spread2.stage3(c)
        norm_chunk(full2, gain2, nrm, c)

    def up(c):
        ffo[...] = lax.dot_general(nrm[...], wff[...], NT, preferred_element_type=F32)

    def act(c):
        base = c * CH

        def body(i, carry):
            r = pl.multiple_of(i * 16, 16)
            rows = pl.ds(r, 16)
            hid[pl.ds(base + r, 16), :] = (jax.nn.silu(ffo[rows, :FFL]) * ffo[rows, FP:]).astype(BF16)
            return carry

        lax.fori_loop(0, CH // 16, body, 0, unroll=2)

    def products(rows, side):
        for target in range(SIDE):
            own_columns = pl.ds(pl.multiple_of((2 * target + side) * CB, CB), CB)
            part2[target, side, rows, :] = jnp.dot(
                hid[rows, :], wd[:, own_columns], preferred_element_type=F32
            ).astype(BF16)

    def down(c):
        rows = pl.ds(c * CH, CH)
        products(rows, 1 - core)
        sum2.stage0(c)

    def keep(c):
        products(pl.ds(c * CH, CH), core)

    def finish(c):
        rows = pl.ds(c * CH, CH)
        layer_out = (full2[tp, rows, :].astype(F32) + sum2.stage3(c)).astype(BF16)
        ordered = jnp.dot(perm[...], layer_out, preferred_element_type=F32).astype(BF16)
        for s in range(SEQS):
            out[pl.ds(s * LEN + c * STEPS, STEPS), :] = ordered[s * STEPS : (s + 1) * STEPS]

    local[3].wait()
    g_wo.own()
    spread1.stage0(3)
    spread1.stage0(1)
    spread1.stage0(0)
    spread1.stage0(2)
    g_wgi.own()
    g_wo.near()
    small_operands()
    g_wgi.near()
    g_wgi.far()
    g_wo.far()
    spread1.stage1(0)
    g_wgi.relay(1)
    g_wgi.relay(2)
    g_wgi.relay(0)
    spread1.stage1(1)
    g_wgi.relay(3)
    spread1.stage1(2)
    g_wo.relay(0)
    g_wo.relay(3)
    spread1.stage1(3)
    spread1.stage2(1)
    g_wo.relay(2)
    g_wo.relay(1)
    spread1.stage2(0)
    local[6].wait()
    g_wd.own()
    local[4].wait()
    local[5].wait()
    g_wff.own()
    norm1(0)
    g_wgi.done()
    project(0)
    spread1.stage2(2)
    scan(0)
    g_wo.done()
    mix_out(0)
    norm1(1)
    project(1)
    sum1.stage1(0)
    scan(1)
    mix_out(1)
    spread1.stage2(3)
    norm1(2)
    sum1.stage1(1)
    g_wff.near()
    sum1.stage2(0)
    project(2)
    norm1(3)
    scan(2)
    sum1.stage2(1)
    g_wff.relay(0)
    project(3)
    mix_out(2)
    settle(0)
    g_wff.far()
    sum1.stage1(2)
    settle(1)
    sum1.stage2(2)
    g_wff.relay(2)
    scan(3)
    spread2.stage1(1)
    g_wff.relay(1)
    mix_out(3)
    spread2.stage1(0)
    g_wff.relay(3)
    sum1.stage1(3)
    g_wgi.drain()
    g_wo.drain()
    settle(2)
    spread1.drain()
    g_wd.near()
    spread2.stage2(1)
    spread2.stage2(0)
    norm2(0)
    sum1.stage2(3)
    g_wff.done()
    up(0)
    spread2.stage1(2)
    g_wd.far()
    g_wd.relay(0)
    g_wd.relay(1)
    act(0)
    norm2(1)
    settle(3)
    up(1)
    g_wd.relay(2)
    spread2.stage2(2)
    g_wd.relay(3)
    act(1)
    norm2(2)
    up(2)
    act(2)
    spread2.stage1(3)
    g_wd.done()
    down(0)
    down(1)
    keep(0)
    sum2.stage1(0)
    keep(1)
    sum2.stage1(1)
    down(2)
    keep(2)
    spread2.stage2(3)
    sum2.stage1(2)
    norm2(3)
    g_wff.drain()
    sum2.stage2(0)
    sum2.stage2(1)
    up(3)
    act(3)
    down(3)
    keep(3)
    sum2.stage1(3)
    sum2.stage2(2)
    perm[...] = order((CH, CH), "sequence")
    finish(1)
    spread2.drain()
    sum2.stage2(3)
    g_wd.drain()
    finish(0)
    sum1.drain(full1)
    finish(2)
    finish(3)

    sum2.drain(full2)


def layer(*operands):
    sums = [
        pltpu.VMEM((SIDE, 2, ROWS, CB), BF16),
        pltpu.VMEM((SIDE, ROWS, CB), BF16),
        pltpu.VMEM((SIDE, ROWS, CB), BF16),
        pltpu.VMEM((2, CHUNKS, HALF, CB), BF16),
        pltpu.VMEM((2, ROWS, CB), BF16),
    ]
    return pl.pallas_call(
        kernel,
        out_shape=jax.ShapeDtypeStruct((ROWS, CB), BF16),
        in_specs=[pl.BlockSpec(memory_space=pl.ANY)] * len(operands),
        out_specs=pl.BlockSpec(memory_space=pltpu.VMEM),
        scratch_shapes=[
            pltpu.VMEM((8, ROWS, CB), BF16),
            pltpu.VMEM((8, ROWS, CB), BF16),
            pltpu.VMEM((2 * RP, 2048), BF16),
            pltpu.VMEM((RP, 2048), BF16),
            pltpu.VMEM((FP + FFL, 2048), BF16),
            pltpu.VMEM((FFL, 2048), BF16),
            *sums,
            *sums,
            pltpu.VMEM((ROWS, CB), BF16),
            pltpu.VMEM((R, R), BF16),
            pltpu.VMEM((R, R), BF16),
            pltpu.VMEM((4, R), F32),
            pltpu.VMEM((R,), F32),
            pltpu.VMEM((SEQS, LEN), F32),
            pltpu.VMEM((16, 128), F32),
            pltpu.VMEM((16, 128), F32),
            pltpu.VMEM((RP, 2 * RP), BF16),
            pltpu.VMEM((8, RP), F32),
            pltpu.VMEM((ROWS, 128), F32),
            pltpu.VMEM((CH, CH), BF16),
            pltpu.VMEM((24 + ROWS, RP), F32),
            pltpu.VMEM((CH, RP), F32),
            pltpu.VMEM((CH, RP), BF16),
            pltpu.VMEM((CH, 2 * RP), F32),
            pltpu.VMEM((CH, RP), BF16),
            pltpu.VMEM((CH, 2048), BF16),
            pltpu.VMEM((CH, FP + FFL), F32),
            pltpu.VMEM((ROWS, FFL), BF16),
            pltpu.VMEM((SEQS, RP), F32),
            pltpu.SemaphoreType.DMA((14,)),
            pltpu.SemaphoreType.DMA((4,)),
            pltpu.SemaphoreType.DMA((4, 7)),
            pltpu.SemaphoreType.DMA((2,)),
            pltpu.SemaphoreType.DMA((2, 3, CHUNKS)),
            pltpu.SemaphoreType.DMA((2,)),
            pltpu.SemaphoreType.DMA((2, 3, CHUNKS)),
        ],
        compiler_params=pltpu.CompilerParams(
            collective_id=0, has_side_effects=True, vmem_limit_bytes=66_000_000
        ),
    )(*operands)


def shards(
    tokens,
    recurrence_norm_gain,
    output_gate_weight,
    recurrence_input_weight,
    convolution_taps,
    recurrence_gate_weight,
    input_gate_weight,
    base_decay_logit,
    token_log_decay,
    recurrence_output_weight,
    feedforward_norm_gain,
    feedforward_gate_weight,
    feedforward_up_weight,
    feedforward_down_weight,
):
    return layer(
        output_gate_weight.T,
        recurrence_input_weight.T,
        tokens,
        recurrence_output_weight,
        feedforward_gate_weight.T,
        feedforward_up_weight.T,
        feedforward_down_weight,
        recurrence_gate_weight.reshape(R, R),
        input_gate_weight.reshape(R, R),
        convolution_taps,
        base_decay_logit,
        token_log_decay.reshape(SEQS, LEN),
        recurrence_norm_gain.reshape(16, 128),
        feedforward_norm_gain.reshape(16, 128),
    )


def solution(mesh):
    in_specs = (
        P("fs", "tp"),
        P(),
        P("fs", "tp"),
        P("fs", "tp"),
        P(None, "tp"),
        P("tp", None, None),
        P("tp", None, None),
        P("tp"),
        P("fs"),
        P("tp", "fs"),
        P(),
        P("fs", "tp"),
        P("fs", "tp"),
        P("tp", "fs"),
    )
    return jax.shard_map(shards, mesh=mesh, in_specs=in_specs, out_specs=P("fs", "tp"), check_vma=False)
```
